32 devices in a mesh: sp: 4 (over z), fs: 4 (over y, x), tp: 2 (over core).
Axes of the slice: x: 2, y: 2, z: 4, core: 2. Of those that a mesh axis runs over, the one named last changes fastest.
Arguments:
- tokens: bfloat16 [4, 1024, 2048], P('fs', 'sp'), may hold values from -6 to 6
- norm_gain: float32 [2048], replicated, may hold values from 0.1 to 1.9
- pool_input: bfloat16 [2048, 2048], P(('sp', 'fs'), 'tp'), may hold values from -0.125 to 0.125
- query_weight: bfloat16 [2048, 2048], P(('sp', 'fs'), 'tp'), may hold values from -20 to 20
- key_weight: bfloat16 [2048, 2048], P(('sp', 'fs'), 'tp'), may hold values from -1 to 1
- value_weight: bfloat16 [2048, 2048], P(('sp', 'fs'), 'tp'), may hold values from -0.125 to 0.125
- pool_map: bfloat16 [8, 256, 256], P('tp'), may hold values from -0.375 to 0.375
- pool_scale: float32 [2048], P('tp'), may hold values from 0.1 to 1.9
- head_gain: float32 [256], replicated, may hold values from 0.1 to 1.9
- diff_lambda: float32 [8], replicated, may hold values from 0.3 to 0.8
- out_pool: bfloat16 [2048, 2048], P('tp', ('sp', 'fs')), may hold values from -0.09375 to 0.09375
- out_heads: bfloat16 [2048, 2048], P('tp', ('sp', 'fs')), may hold values from -0.09375 to 0.09375
Outputs:
- layer_out: bfloat16 [4, 1024, 2048], P('fs', 'sp', 'tp')
The draws below stay inside these ranges and needn't reach their ends.
All inputs are finite; a program needn't handle non-finite values.
Results may differ from the reference program's by a relative error of at most 0.018.
Values may be sent and summed in bfloat16 or wider, within the bound.
No kernel may reach another device: no remote copies, remote signals or barrier semaphores. Data moves between devices by JAX's collectives and lax.ppermute only.
A program may use at most 64 MiB of HBM per device.

```python
import math
import jax
import jax.numpy as jnp
from jax import lax

D = 2048
HEADS = 8
HEAD_DIM = 128
POOL_GROUPS = 8
GROUP_DIM = 256
POOL_WIDTH = 2048
SEQ = 1024
SEQS = 4
N_TP = 2


def key_matrix(key):
    normal_part = jax.random.truncated_normal(jax.random.fold_in(key, 11), -6.0, 6.0, (D, 2 * HEADS * HEAD_DIM), jnp.float32)
    return normal_part * D ** (-0.5)


def draw_key_weight(key, part):
    return key_matrix(key).astype(jnp.bfloat16)


def draw_query_weight(key, part):
    normal_part = jax.random.truncated_normal(jax.random.fold_in(key, 12), -6.0, 6.0, (D, 2 * HEADS * HEAD_DIM), jnp.float32)
    result = normal_part * (3.0 / D) ** 0.5
    return result.astype(jnp.bfloat16)


def levels(key, shape, cuts, smallest, high):
    loudness, own = 1.0, jax.random.fold_in(key, 6)
    for dim, shards_of in cuts:
        draws = jnp.exp(jax.random.uniform(jax.random.fold_in(own, dim), (shards_of,), jnp.float32, smallest / len(cuts), high / len(cuts)))
        loudness = loudness * jnp.repeat(draws, shape[dim] // shards_of).reshape([-1 if axis == dim else 1 for axis in range(len(shape))])
    return loudness


def normal_values(key, extent, spread, limit, split=(), kind=jnp.bfloat16):
    array = jax.random.normal(key, extent, jnp.float32) * spread
    if len(split) > 0:
        array = levels(key, extent, split, -0.22, 0.18) * array
    return jnp.clip(array, min=-limit, max=limit).astype(kind)


def setup_inputs(seed: int = 0) -> dict:
    arg_keys = jax.random.split(jax.random.key(seed), 13)
    return {
        "tokens": normal_values(arg_keys[0], (SEQS, SEQ, D), 1.0, 6.0, ((0, 4), (1, 4))),
        "norm_gain": jnp.clip(1.0 + 0.18 * jax.random.normal(arg_keys[1], (D,), jnp.float32), 0.1, 1.9),
        "pool_input": normal_values(arg_keys[2], (D, POOL_WIDTH), D ** -0.5, 0.125, ((0, 16), (1, 2))),
        "query_weight": draw_query_weight(jax.random.fold_in(arg_keys[12], 71), 0),
        "key_weight": draw_key_weight(jax.random.fold_in(arg_keys[12], 71), 0),
        "value_weight": normal_values(arg_keys[5], (D, 2 * HEADS * HEAD_DIM), D ** -0.5, 0.125, ((0, 16), (1, 2))),
        "pool_map": normal_values(arg_keys[6], (POOL_GROUPS, GROUP_DIM, GROUP_DIM), GROUP_DIM ** -0.5, 0.375, ((0, 2),)),
        "pool_scale": jnp.clip(1.0 + 0.18 * jax.random.normal(arg_keys[7], (POOL_WIDTH,), jnp.float32), 0.1, 1.9),
        "head_gain": jnp.clip(1.0 + 0.18 * jax.random.normal(arg_keys[8], (2 * HEAD_DIM,), jnp.float32), 0.1, 1.9),
        "diff_lambda": jnp.clip(jax.random.uniform(arg_keys[9], (HEADS,), jnp.float32, 0.3, 0.8), 0.3, 0.8),
        "out_pool": normal_values(arg_keys[10], (POOL_WIDTH, D), (POOL_WIDTH + 2 * HEADS * HEAD_DIM) ** -0.5, 0.09375, ((0, 2), (1, 16))),
        "out_heads": normal_values(arg_keys[11], (2 * HEADS * HEAD_DIM, D), (POOL_WIDTH + 2 * HEADS * HEAD_DIM) ** -0.5, 0.09375, ((0, 2), (1, 16))),
    }


THETA = 500000.0
HEAD_SCALE = 0.8
NORM_EPS = 1e-06
HEAD_EPS = 1e-05

def rotate(tensor, positions):
    half = HEAD_DIM // 2
    freqs = 1.0 / THETA ** (jnp.arange(half, dtype=jnp.float32) * 2.0 / HEAD_DIM)
    angles = positions[:, None] * freqs[None, :]
    cosine = jnp.cos(angles)[:, None, None, :]
    sine = jnp.sin(angles)[:, None, None, :]
    floated = tensor.astype(jnp.float32)
    first = floated[..., :half]
    second = floated[..., half:]
    turned = jnp.concatenate([first * cosine - second * sine, second * cosine + first * sine], -1)
    return turned.astype(jnp.bfloat16)

def one_sequence(seq_tokens, norm_gain, pool_input, query_weight, key_weight, value_weight, pool_map, pool_scale, head_gain, diff_lambda, out_pool, out_heads):
    length = seq_tokens.shape[0]
    floated = seq_tokens.astype(jnp.float32)
    normed = (floated * lax.rsqrt(lax.optimization_barrier(jnp.mean(floated * floated, -1, keepdims=True)) + NORM_EPS) * norm_gain).astype(jnp.bfloat16)
    pool_in = jnp.dot(normed, pool_input, preferred_element_type=jnp.float32).astype(jnp.bfloat16)
    queries = jnp.dot(normed, query_weight, preferred_element_type=jnp.float32).astype(jnp.bfloat16)
    keys_all = jnp.dot(normed, key_weight, preferred_element_type=jnp.float32).astype(jnp.bfloat16)
    values = jnp.dot(normed, value_weight, preferred_element_type=jnp.float32).astype(jnp.bfloat16)
    positions = jnp.arange(length, dtype=jnp.float32)
    queries = rotate(queries.reshape(length, HEADS, 2, HEAD_DIM), positions)
    keys_all = rotate(keys_all.reshape(length, HEADS, 2, HEAD_DIM), positions)
    values = values.reshape(length, HEADS, 2 * HEAD_DIM)
    span = math.gcd(length, 512)

    def one_head(operands):
        query_head, key_head, value_head, lambda_head = operands
        key_float = key_head.astype(jnp.float32)
        value_float = value_head.astype(jnp.float32)

        def one_block(begin):
            query_block = lax.dynamic_slice_in_dim(query_head, begin, span, 0).astype(jnp.float32)
            scores = jnp.einsum('qcd,kcd->cqk', query_block, key_float) * HEAD_DIM ** (-0.5)
            query_pos = begin + jnp.arange(span, dtype=jnp.int32)
            key_pos = jnp.arange(length, dtype=jnp.int32)
            scores = jnp.where(query_pos[:, None] >= key_pos[None, :], scores, -jnp.inf)
            largest = lax.optimization_barrier(jnp.max(scores, -1, keepdims=True))
            expons = jnp.exp(scores - largest)
            totals = lax.optimization_barrier(jnp.sum(expons, -1))
            expons_low = expons.astype(jnp.bfloat16).astype(jnp.float32)
            map_values = jnp.einsum('cqk,ke->cqe', expons_low, value_float)
            return map_values[0] / totals[0][:, None] - lambda_head * map_values[1] / totals[1][:, None]
        begins = jnp.arange(length // span, dtype=jnp.int32) * span
        return lax.map(one_block, begins).reshape(length, 2 * HEAD_DIM)
    heads_raw = lax.map(one_head, (jnp.moveaxis(queries, 1, 0), jnp.moveaxis(keys_all, 1, 0), jnp.moveaxis(values, 1, 0), diff_lambda))
    heads_raw = jnp.moveaxis(heads_raw, 0, 1)
    attn = (heads_raw * lax.rsqrt(lax.optimization_barrier(jnp.mean(heads_raw * heads_raw, -1, keepdims=True)) + HEAD_EPS) * head_gain * HEAD_SCALE).astype(jnp.bfloat16).reshape(length, 2 * HEADS * HEAD_DIM)
    grouped = pool_in.reshape(length, POOL_GROUPS, GROUP_DIM).astype(jnp.float32)
    running = jnp.concatenate([jnp.zeros((1, POOL_GROUPS, GROUP_DIM), jnp.float32), jnp.cumsum(grouped, 0)], 0)
    windows = 2 ** (1 + jnp.arange(POOL_GROUPS, dtype=jnp.int32) % 4)
    places = jnp.arange(length, dtype=jnp.int32)[:, None]
    lowest = jnp.maximum(places + 1 - windows[None, :], 0)
    counts = jnp.minimum(places + 1, windows[None, :]).astype(jnp.float32)
    low_sums = running[lowest, jnp.arange(POOL_GROUPS, dtype=jnp.int32)[None, :]]
    window_mean = (running[1:] - low_sums) / counts[:, :, None]
    pool_mixed = (window_mean - grouped).astype(jnp.bfloat16)
    pooled = (jnp.einsum('sgc,gce->sge', pool_mixed.astype(jnp.float32), pool_map.astype(jnp.float32)) * pool_scale.reshape(POOL_GROUPS, GROUP_DIM)).astype(jnp.bfloat16).reshape(length, POOL_WIDTH)
    pool_cols = POOL_WIDTH // N_TP
    head_cols = 2 * HEADS * HEAD_DIM // N_TP
    summed = jnp.zeros((length, D), jnp.float32)
    for shard_index in range(N_TP):
        pool_part = pooled[:, shard_index * pool_cols:(shard_index + 1) * pool_cols]
        head_part = attn[:, shard_index * head_cols:(shard_index + 1) * head_cols]
        partial_value = jnp.dot(pool_part, out_pool[shard_index * pool_cols:(shard_index + 1) * pool_cols], preferred_element_type=jnp.float32) + jnp.dot(head_part, out_heads[shard_index * head_cols:(shard_index + 1) * head_cols], preferred_element_type=jnp.float32)
        rounded = lax.optimization_barrier(partial_value.astype(jnp.bfloat16))
        summed = summed + rounded.astype(jnp.float32)
    return summed.astype(jnp.bfloat16)

def reference(tokens, norm_gain, pool_input, query_weight, key_weight, value_weight, pool_map, pool_scale, head_gain, diff_lambda, out_pool, out_heads):

    def apply_one(seq_tokens):
        return one_sequence(seq_tokens, norm_gain, pool_input, query_weight, key_weight, value_weight, pool_map, pool_scale, head_gain, diff_lambda, out_pool, out_heads)
    return lax.map(apply_one, tokens)
```

```python
import functools
import math

import jax
import jax.numpy as jnp
from jax import lax
from jax.experimental import pallas as pl
from jax.experimental.pallas import tpu as pltpu
from jax.sharding import PartitionSpec as P

HEAD_DIM = 128
GROUP_DIM = 256


THETA = 500000.0
HEAD_SCALE = 0.8
NORM_EPS = 1e-06
HEAD_EPS = 1e-05


def from_behind(value, axis, steps):
    count = lax.axis_size(axis)
    first, last = (max(0, -steps), min(count, count - steps))
    return lax.ppermute(value, axis, [(source, source + steps) for source in range(first, last)])


def rotate(tensor, positions):
    half = HEAD_DIM // 2
    freqs = 1.0 / THETA ** (jnp.arange(half, dtype=jnp.float32) * 2.0 / HEAD_DIM)
    angles = positions[:, None] * freqs[None, :]
    cosine = jnp.cos(angles)[:, None, None, :]
    sine = jnp.sin(angles)[:, None, None, :]
    floated = tensor.astype(jnp.float32)
    first = floated[..., :half]
    second = floated[..., half:]
    turned = jnp.concatenate([first * cosine - second * sine, second * cosine + first * sine], -1)
    return turned.astype(jnp.bfloat16)


def local(
    tokens,
    norm_gain,
    pool_input,
    query_weight,
    key_weight,
    value_weight,
    pool_map,
    pool_scale,
    head_gain,
    diff_lambda,
    out_pool,
    out_heads,
):
    out_local = jnp.concatenate([out_pool, out_heads], 0)
    row_count = tokens.shape[1]
    floated = tokens[0].astype(jnp.float32)
    normed = (
        floated * lax.rsqrt(jnp.mean(floated * floated, -1, keepdims=True) + NORM_EPS) * norm_gain
    ).astype(jnp.bfloat16)
    fragments = (
        lax.all_gather(pool_input, ("sp", "fs"), axis=0, tiled=True),
        lax.all_gather(query_weight, ("sp", "fs"), axis=0, tiled=True),
        lax.all_gather(key_weight, ("sp", "fs"), axis=0, tiled=True),
        lax.all_gather(value_weight, ("sp", "fs"), axis=0, tiled=True),
    )
    projected = tuple(
        (jnp.dot(normed, fragment, preferred_element_type=jnp.float32) for fragment in fragments)
    )
    pool_in, queries, keys_flat, values_flat = [
        product.astype(jnp.bfloat16) for product in projected
    ]
    head_count = values_flat.shape[1] // (2 * HEAD_DIM)
    tp_index = lax.axis_index("tp")
    sp_index = lax.axis_index("sp")
    query_pos = sp_index * row_count + jnp.arange(row_count, dtype=jnp.int32)
    positions = query_pos.astype(jnp.float32)
    queries = rotate(queries.reshape(row_count, head_count, 2, HEAD_DIM), positions)
    keys_flat = rotate(keys_flat.reshape(row_count, head_count, 2, HEAD_DIM), positions).reshape(
        row_count, head_count * 2 * HEAD_DIM
    )
    lambdas = lax.dynamic_slice_in_dim(diff_lambda, tp_index * head_count, head_count, 0)

    def online_step(state, key_rows, value_rows, key_offset):
        largest, summed, accum = state
        width = key_rows.shape[0]
        shaped = key_rows.reshape(width, head_count, 2, HEAD_DIM)
        scores = jnp.einsum(
            "qhcd,khcd->chqk", queries, shaped, preferred_element_type=jnp.float32
        ) * HEAD_DIM ** (-0.5)
        key_pos = key_offset + jnp.arange(width, dtype=jnp.int32)
        scores = jnp.where(query_pos[:, None] >= key_pos[None, :], scores, -jnp.inf)
        newest = jnp.maximum(largest, jnp.max(scores, -1))
        anchor = jnp.where(jnp.isfinite(newest), newest, 0.0)
        rescale = jnp.exp(largest - anchor)
        expons = jnp.exp(scores - anchor[..., None])
        summed = summed * rescale + jnp.sum(expons, -1)
        value_shaped = value_rows.reshape(width, head_count, 2 * HEAD_DIM)
        added = jnp.einsum(
            "chqk,khe->chqe",
            expons.astype(jnp.bfloat16),
            value_shaped,
            preferred_element_type=jnp.float32,
        )
        accum = accum * rescale[..., None] + added
        return (newest, summed, accum)

    start_state = (
        jnp.full((2, head_count, row_count), -jnp.inf, jnp.float32),
        jnp.zeros((2, head_count, row_count), jnp.float32),
        jnp.zeros((2, head_count, row_count, 2 * HEAD_DIM), jnp.float32),
    )
    fragments = (
        lax.all_gather(keys_flat, "sp", axis=0, tiled=True),
        lax.all_gather(values_flat, "sp", axis=0, tiled=True),
    )
    span = math.gcd(fragments[0].shape[0], 1024)

    def inner_step(index, inner_state):
        key_rows = lax.dynamic_slice_in_dim(fragments[0], index * span, span, 0)
        value_rows = lax.dynamic_slice_in_dim(fragments[1], index * span, span, 0)
        return online_step(inner_state, key_rows, value_rows, index * span)

    final_state = lax.fori_loop(0, fragments[0].shape[0] // span, inner_step, start_state)
    summed_final = final_state[1]
    accum_final = final_state[2]
    heads_raw = (
        accum_final[0] / summed_final[0][..., None]
        - lambdas[:, None, None] * accum_final[1] / summed_final[1][..., None]
    )
    heads_raw = jnp.moveaxis(heads_raw, 0, 1)
    attn = (
        (
            heads_raw
            * lax.rsqrt(jnp.mean(heads_raw * heads_raw, -1, keepdims=True) + HEAD_EPS)
            * head_gain
            * HEAD_SCALE
        )
        .astype(jnp.bfloat16)
        .reshape(row_count, head_count * 2 * HEAD_DIM)
    )
    reach = 15
    rim_rows = from_behind(pool_in[row_count - reach :], "sp", 1)
    extended = jnp.concatenate([rim_rows, pool_in], 0).astype(jnp.float32)
    pair_sums = extended[1:] + extended[:-1]
    quad_sums = pair_sums[2:] + pair_sums[:-2]
    octet_sums = quad_sums[4:] + quad_sums[:-4]
    sixteen_sums = octet_sums[8:] + octet_sums[:-8]
    group_count = pool_in.shape[1] // GROUP_DIM
    stacked = jnp.stack(
        [
            pair_sums[14 : 14 + row_count],
            quad_sums[12 : 12 + row_count],
            octet_sums[8 : 8 + row_count],
            sixteen_sums,
        ],
        0,
    ).reshape(4, row_count, group_count, GROUP_DIM)
    levels = (tp_index * group_count + jnp.arange(group_count, dtype=jnp.int32)) % 4
    picked = jnp.sum(
        jnp.where(
            levels[None, None, :, None] == jnp.arange(4, dtype=jnp.int32)[:, None, None, None],
            stacked,
            0.0,
        ),
        0,
    )
    windows = 2 ** (1 + levels)
    counts = jnp.minimum(query_pos[:, None] + 1, windows[None, :]).astype(jnp.float32)
    window_mean = picked / counts[:, :, None]
    grouped = pool_in.reshape(row_count, group_count, GROUP_DIM).astype(jnp.float32)
    pool_mixed = (window_mean - grouped).astype(jnp.bfloat16)
    pooled = (
        (
            jnp.einsum("tgc,gce->tge", pool_mixed, pool_map, preferred_element_type=jnp.float32)
            * pool_scale.reshape(group_count, GROUP_DIM)
        )
        .astype(jnp.bfloat16)
        .reshape(row_count, group_count * GROUP_DIM)
    )
    branches = jnp.concatenate([pooled, attn], 1)
    partial_value = jnp.dot(
        branches,
        lax.all_gather(out_local, ("sp", "fs"), axis=1, tiled=True),
        preferred_element_type=jnp.float32,
    )
    layer_out = lax.psum_scatter(
        partial_value.astype(jnp.bfloat16), "tp", scatter_dimension=1, tiled=True
    )
    return layer_out[None]


def mix_kernel(meta_ref, proj_ref, cos_ref, sin_ref, map_ref, scale_ref, gain_ref, lam_ref, out_ref, keys_ref):
    rows = out_ref.shape[0]
    length = proj_ref.shape[0]
    width = 2 * HEAD_DIM
    step = pl.program_id(0)
    first_pos = meta_ref[0]
    level = meta_ref[1]

    def turned(raw, cosine, sine):
        raw = raw.astype(jnp.float32)
        return (raw * cosine + pltpu.roll(raw, HEAD_DIM // 2, 1) * sine).astype(jnp.bfloat16)

    @pl.when(step == 0)
    def _():
        for m in range(2):
            begin = GROUP_DIM + width + m * HEAD_DIM
            keys_ref[:, m * HEAD_DIM : (m + 1) * HEAD_DIM] = turned(
                proj_ref[:, begin : begin + HEAD_DIM], cos_ref[...], sin_ref[...]
            )

    base = pl.multiple_of(step * rows, rows)
    mine = pl.ds(base, rows)
    start_pos = lax.rem(first_pos + base, length)
    key_index = lax.broadcasted_iota(jnp.int32, (rows, length), 1)
    key_pos = lax.rem(key_index + first_pos, length)
    query_pos = start_pos + lax.broadcasted_iota(jnp.int32, (rows, length), 0)
    allowed = query_pos >= key_pos
    value = proj_ref[:, GROUP_DIM + 2 * width : GROUP_DIM + 3 * width]
    halves = []
    for m in range(2):
        begin = GROUP_DIM + m * HEAD_DIM
        query = turned(proj_ref[mine, begin : begin + HEAD_DIM], cos_ref[mine, :], sin_ref[mine, :])
        scores = lax.dot_general(
            query,
            keys_ref[:, m * HEAD_DIM : (m + 1) * HEAD_DIM],
            (((1,), (1,)), ((), ())),
            preferred_element_type=jnp.float32,
        ) * HEAD_DIM ** (-0.5)
        scores = jnp.where(allowed, scores, -jnp.inf)
        largest = jnp.max(scores, -1, keepdims=True)
        expons = jnp.exp(scores - largest)
        total = jnp.sum(expons, -1, keepdims=True)
        summed = jnp.dot(expons.astype(jnp.bfloat16), value, preferred_element_type=jnp.float32)
        halves.append(summed / total)
    raw = halves[0] - lam_ref[0] * halves[1]
    attn = (
        raw
        * lax.rsqrt(jnp.mean(raw * raw, -1, keepdims=True) + HEAD_EPS)
        * gain_ref[...]
        * HEAD_SCALE
    ).astype(jnp.bfloat16)
    out_ref[:, GROUP_DIM:] = attn

    reach = 16
    before = pl.multiple_of(lax.rem(base + length - reach, length), reach)
    pos = start_pos - reach + lax.broadcasted_iota(jnp.int32, (rows + reach, GROUP_DIM), 0)
    flat = jnp.concatenate(
        [proj_ref[pl.ds(before, reach), :GROUP_DIM], proj_ref[mine, :GROUP_DIM]], 0
    ).astype(jnp.float32)
    flat = jnp.where(pos >= 0, flat, 0.0)
    sums = flat
    picked = jnp.zeros((rows, GROUP_DIM), jnp.float32)
    for power in range(4):
        sums = sums + pltpu.roll(sums, 2**power, 0)
        picked = jnp.where(level == power, sums[reach:], picked)
    window = lax.shift_left(jnp.int32(2), level)
    own_pos = pos[reach:]
    counts = jnp.minimum(own_pos + 1, window).astype(jnp.float32)
    mixed = (picked / counts - flat[reach:]).astype(jnp.bfloat16)
    pooled = jnp.dot(mixed, map_ref[...], preferred_element_type=jnp.float32) * scale_ref[...]
    out_ref[:, :GROUP_DIM] = pooled.astype(jnp.bfloat16)


def mix(meta, proj, cosine, sine, pool_map, pool_scale, head_gain, lam, blocks):
    length = proj.shape[0]
    rows = length // blocks
    whole = lambda i, *_: (0, 0)
    return pl.pallas_call(
        mix_kernel,
        out_shape=jax.ShapeDtypeStruct((length, GROUP_DIM + 2 * HEAD_DIM), jnp.bfloat16),
        grid_spec=pltpu.PrefetchScalarGridSpec(
            num_scalar_prefetch=1,
            grid=(blocks,),
            in_specs=[
                pl.BlockSpec(proj.shape, whole),
                pl.BlockSpec(cosine.shape, whole),
                pl.BlockSpec(sine.shape, whole),
                pl.BlockSpec(pool_map.shape, whole),
                pl.BlockSpec(pool_scale.shape, whole),
                pl.BlockSpec(head_gain.shape, whole),
                pl.BlockSpec(memory_space=pltpu.SMEM),
            ],
            out_specs=pl.BlockSpec((rows, GROUP_DIM + 2 * HEAD_DIM), lambda i, *_: (i, 0)),
            scratch_shapes=[pltpu.VMEM((length, 2 * HEAD_DIM), jnp.bfloat16)],
        ),
        compiler_params=pltpu.CompilerParams(dimension_semantics=("arbitrary",)),
        cost_estimate=pl.CostEstimate(
            flops=8 * length * length * HEAD_DIM, bytes_accessed=3 * proj.size, transcendentals=2 * length * length
        ),
        name="mix",
    )(meta, proj, cosine, sine, pool_map, pool_scale, head_gain, lam)


def fold_rows(value):
    return value.reshape(-1, value.shape[-1])


def swap(value, axis, bits):
    return lax.ppermute(value, axis, [(i, i ^ bits) for i in range(lax.axis_size(axis))])


def shift(value, axis, up, sources):
    step = 1 if up else -1
    return lax.ppermute(value, axis, [(i, i + step) for i in sources])


def gather_square(block):
    half = block.shape[0] // 2
    one, two = swap(block, "fs", 1), swap(block, "fs", 2)
    three = jnp.concatenate([swap(two[:half], "fs", 1), swap(one[half:], "fs", 2)], 0)
    return [block, one, two, three]


def spread(
    tokens,
    norm_gain,
    pool_input,
    query_weight,
    key_weight,
    value_weight,
    pool_map,
    pool_scale,
    head_gain,
    diff_lambda,
    out_pool,
    out_heads,
):
    n_sp, n_fs, n_tp = (lax.axis_size(axis) for axis in ("sp", "fs", "tp"))
    sp, fs, tp = (lax.axis_index(axis) for axis in ("sp", "fs", "tp"))
    rows, depth = tokens.shape[1:]
    length = rows * n_sp
    shard = depth // (n_sp * n_fs)

    packed = jnp.stack(
        [w.reshape(shard, n_sp, -1) for w in (pool_input, query_weight, key_weight, value_weight)], 2
    )
    packed = jnp.moveaxis(packed, 1, 0).reshape(n_sp, shard, -1)
    arrived = fold_rows(lax.all_to_all(packed, "sp", 0, 0, tiled=True))
    weight = jnp.concatenate(gather_square(arrived), 0)

    floated = tokens[0].astype(jnp.float32)
    normed = (
        floated * lax.rsqrt(jnp.mean(floated * floated, -1, keepdims=True) + NORM_EPS) * norm_gain
    ).astype(jnp.bfloat16)
    split = normed.reshape(rows, n_sp, n_fs, shard)
    own = jnp.concatenate(
        [lax.dynamic_index_in_dim(split, fs ^ j, 2, False) for j in range(n_fs)], 1
    ).reshape(rows, depth)
    half = rows // n_tp
    mine = lax.dynamic_slice_in_dim(own, tp * half, half, 0)
    up, down = [mine], [mine]
    for k in range(1, n_sp):
        up.append(shift(up[-1], "sp", True, range(k - 1, n_sp - 1)))
        down.append(shift(down[-1], "sp", False, range(1, n_sp + 1 - k)))
    blocks = []
    for k in range(n_sp - 1, 0, -1):
        here = up[k] + down[n_sp - k]
        there = swap(here, "tp", 1)
        blocks += [jnp.where(tp == 0, here, there), jnp.where(tp == 0, there, here)]
    sequence = jnp.concatenate(blocks + [own], 0)

    proj = jnp.dot(sequence, weight, preferred_element_type=jnp.float32).astype(jnp.bfloat16)

    first_pos = lax.rem((sp + 1) * rows, length)
    positions = lax.rem(first_pos + jnp.arange(length, dtype=jnp.int32), length).astype(jnp.float32)
    freqs = 1.0 / THETA ** (jnp.arange(HEAD_DIM // 2, dtype=jnp.float32) * 2.0 / HEAD_DIM)
    angles = positions[:, None] * freqs[None, :]
    cosine, sine = jnp.cos(angles), jnp.sin(angles)
    group = tp * n_sp + sp
    meta = jnp.stack([first_pos, lax.rem(group, 4)]).astype(jnp.int32)
    branches = mix(
        meta,
        proj,
        jnp.concatenate([cosine, cosine], 1),
        jnp.concatenate([-sine, sine], 1),
        lax.dynamic_index_in_dim(pool_map, sp, 0, False),
        lax.dynamic_slice_in_dim(pool_scale, sp * GROUP_DIM, GROUP_DIM, 0)[None],
        head_gain[None],
        lax.dynamic_slice_in_dim(diff_lambda, group, 1, 0),
        n_sp,
    )

    packed_out = jnp.concatenate(
        [out_pool.reshape(n_sp, GROUP_DIM, shard), out_heads.reshape(n_sp, 2 * HEAD_DIM, shard)], 1
    )
    channels = packed_out.shape[1]
    arrived_out = fold_rows(lax.all_to_all(packed_out, "sp", 0, 0, tiled=True))
    pieces = [p.reshape(n_tp, n_sp // n_tp, channels, shard) for p in gather_square(arrived_out)]
    out_weight = jnp.stack(pieces, 1)
    out_weight = jnp.moveaxis(out_weight, 3, 1).reshape(n_tp, channels, depth // n_tp)
    kept_weight = lax.dynamic_index_in_dim(out_weight, tp, 0, False)
    sent_weight = lax.dynamic_index_in_dim(out_weight, 1 - tp, 0, False)

    def block_sum(k):
        part = branches[(n_sp - 1 - k) * rows : (n_sp - k) * rows]
        sent = jnp.dot(part, sent_weight, preferred_element_type=jnp.float32).astype(jnp.bfloat16)
        kept = jnp.dot(part, kept_weight, preferred_element_type=jnp.float32)
        return kept + swap(sent, "tp", 1).astype(jnp.float32)

    sums = {k: block_sum(k) for k in sorted(range(n_sp), key=lambda k: -abs(2 * k - n_sp) if k else 1)}
    rising, falling = (jnp.zeros((rows, depth // n_tp), jnp.bfloat16),) * 2
    for step in range(1, n_sp):
        above = (sums[step] + rising.astype(jnp.float32)).astype(jnp.bfloat16)
        below = (sums[n_sp - step] + falling.astype(jnp.float32)).astype(jnp.bfloat16)
        rising = shift(above, "sp", True, range(0, step))
        falling = shift(below, "sp", False, range(n_sp - step, n_sp))
    result = (sums[0] + rising.astype(jnp.float32) + falling.astype(jnp.float32)).astype(jnp.bfloat16)
    result = result.reshape(rows, n_fs, n_sp // n_tp, shard)
    result = jnp.stack([lax.dynamic_index_in_dim(result, fs ^ j, 1, False) for j in range(n_fs)], 2)
    return result.reshape(1, rows, depth // n_tp)


def solution(mesh):
    placed = (
        P("fs", "sp", None),
        P(),
        P(("sp", "fs"), "tp"),
        P(("sp", "fs"), "tp"),
        P(("sp", "fs"), "tp"),
        P(("sp", "fs"), "tp"),
        P("tp", None, None),
        P("tp"),
        P(),
        P(),
        P("tp", ("sp", "fs")),
        P("tp", ("sp", "fs")),
    )

    def body(*args):
        n_sp, n_fs, n_tp = (mesh.shape[axis] for axis in ("sp", "fs", "tp"))
        groups, heads = args[6].shape[0], args[5].shape[1] // (2 * HEAD_DIM)
        pairs = groups == heads == n_sp and n_fs == 4 and n_tp == 2
        return (spread if pairs else local)(*args)

    return jax.shard_map(
        body, mesh=mesh, in_specs=placed, out_specs=P("fs", "sp", "tp"), check_vma=False
    )
```

```python
import functools
import math

import jax
import jax.numpy as jnp
import numpy as np
from jax import lax
from jax.experimental import pallas as pl
from jax.experimental.pallas import tpu as pltpu
from jax.sharding import PartitionSpec as P


HEAD_DIM = 128
GROUP_DIM = 256


THETA = 500000.0
HEAD_SCALE = 0.8
NORM_EPS = 1e-06
HEAD_EPS = 1e-05


def from_behind(value, axis, steps):
    count = lax.axis_size(axis)
    first, last = (max(0, -steps), min(count, count - steps))
    return lax.ppermute(value, axis, [(source, source + steps) for source in range(first, last)])


def rotate(tensor, positions):
    half = HEAD_DIM // 2
    freqs = 1.0 / THETA ** (jnp.arange(half, dtype=jnp.float32) * 2.0 / HEAD_DIM)
    angles = positions[:, None] * freqs[None, :]
    cosine = jnp.cos(angles)[:, None, None, :]
    sine = jnp.sin(angles)[:, None, None, :]
    floated = tensor.astype(jnp.float32)
    first = floated[..., :half]
    second = floated[..., half:]
    turned = jnp.concatenate([first * cosine - second * sine, second * cosine + first * sine], -1)
    return turned.astype(jnp.bfloat16)


def local(
    tokens,
    norm_gain,
    pool_input,
    query_weight,
    key_weight,
    value_weight,
    pool_map,
    pool_scale,
    head_gain,
    diff_lambda,
    out_pool,
    out_heads,
):
    out_local = jnp.concatenate([out_pool, out_heads], 0)
    row_count = tokens.shape[1]
    floated = tokens[0].astype(jnp.float32)
    normed = (
        floated * lax.rsqrt(jnp.mean(floated * floated, -1, keepdims=True) + NORM_EPS) * norm_gain
    ).astype(jnp.bfloat16)
    fragments = (
        lax.all_gather(pool_input, ("sp", "fs"), axis=0, tiled=True),
        lax.all_gather(query_weight, ("sp", "fs"), axis=0, tiled=True),
        lax.all_gather(key_weight, ("sp", "fs"), axis=0, tiled=True),
        lax.all_gather(value_weight, ("sp", "fs"), axis=0, tiled=True),
    )
    projected = tuple(
        (jnp.dot(normed, fragment, preferred_element_type=jnp.float32) for fragment in fragments)
    )
    pool_in, queries, keys_flat, values_flat = [
        product.astype(jnp.bfloat16) for product in projected
    ]
    head_count = values_flat.shape[1] // (2 * HEAD_DIM)
    tp_index = lax.axis_index("tp")
    sp_index = lax.axis_index("sp")
    query_pos = sp_index * row_count + jnp.arange(row_count, dtype=jnp.int32)
    positions = query_pos.astype(jnp.float32)
    queries = rotate(queries.reshape(row_count, head_count, 2, HEAD_DIM), positions)
    keys_flat = rotate(keys_flat.reshape(row_count, head_count, 2, HEAD_DIM), positions).reshape(
        row_count, head_count * 2 * HEAD_DIM
    )
    lambdas = lax.dynamic_slice_in_dim(diff_lambda, tp_index * head_count, head_count, 0)

    def online_step(state, key_rows, value_rows, key_offset):
        largest, summed, accum = state
        width = key_rows.shape[0]
        shaped = key_rows.reshape(width, head_count, 2, HEAD_DIM)
        scores = jnp.einsum(
            "qhcd,khcd->chqk", queries, shaped, preferred_element_type=jnp.float32
        ) * HEAD_DIM ** (-0.5)
        key_pos = key_offset + jnp.arange(width, dtype=jnp.int32)
        scores = jnp.where(query_pos[:, None] >= key_pos[None, :], scores, -jnp.inf)
        newest = jnp.maximum(largest, jnp.max(scores, -1))
        anchor = jnp.where(jnp.isfinite(newest), newest, 0.0)
        rescale = jnp.exp(largest - anchor)
        expons = jnp.exp(scores - anchor[..., None])
        summed = summed * rescale + jnp.sum(expons, -1)
        value_shaped = value_rows.reshape(width, head_count, 2 * HEAD_DIM)
        added = jnp.einsum(
            "chqk,khe->chqe",
            expons.astype(jnp.bfloat16),
            value_shaped,
            preferred_element_type=jnp.float32,
        )
        accum = accum * rescale[..., None] + added
        return (newest, summed, accum)

    start_state = (
        jnp.full((2, head_count, row_count), -jnp.inf, jnp.float32),
        jnp.zeros((2, head_count, row_count), jnp.float32),
        jnp.zeros((2, head_count, row_count, 2 * HEAD_DIM), jnp.float32),
    )
    fragments = (
        lax.all_gather(keys_flat, "sp", axis=0, tiled=True),
        lax.all_gather(values_flat, "sp", axis=0, tiled=True),
    )
    span = math.gcd(fragments[0].shape[0], 1024)

    def inner_step(index, inner_state):
        key_rows = lax.dynamic_slice_in_dim(fragments[0], index * span, span, 0)
        value_rows = lax.dynamic_slice_in_dim(fragments[1], index * span, span, 0)
        return online_step(inner_state, key_rows, value_rows, index * span)

    final_state = lax.fori_loop(0, fragments[0].shape[0] // span, inner_step, start_state)
    summed_final = final_state[1]
    accum_final = final_state[2]
    heads_raw = (
        accum_final[0] / summed_final[0][..., None]
        - lambdas[:, None, None] * accum_final[1] / summed_final[1][..., None]
    )
    heads_raw = jnp.moveaxis(heads_raw, 0, 1)
    attn = (
        (
            heads_raw
            * lax.rsqrt(jnp.mean(heads_raw * heads_raw, -1, keepdims=True) + HEAD_EPS)
            * head_gain
            * HEAD_SCALE
        )
        .astype(jnp.bfloat16)
        .reshape(row_count, head_count * 2 * HEAD_DIM)
    )
    reach = 15
    rim_rows = from_behind(pool_in[row_count - reach :], "sp", 1)
    extended = jnp.concatenate([rim_rows, pool_in], 0).astype(jnp.float32)
    pair_sums = extended[1:] + extended[:-1]
    quad_sums = pair_sums[2:] + pair_sums[:-2]
    octet_sums = quad_sums[4:] + quad_sums[:-4]
    sixteen_sums = octet_sums[8:] + octet_sums[:-8]
    group_count = pool_in.shape[1] // GROUP_DIM
    stacked = jnp.stack(
        [
            pair_sums[14 : 14 + row_count],
            quad_sums[12 : 12 + row_count],
            octet_sums[8 : 8 + row_count],
            sixteen_sums,
        ],
        0,
    ).reshape(4, row_count, group_count, GROUP_DIM)
    levels = (tp_index * group_count + jnp.arange(group_count, dtype=jnp.int32)) % 4
    picked = jnp.sum(
        jnp.where(
            levels[None, None, :, None] == jnp.arange(4, dtype=jnp.int32)[:, None, None, None],
            stacked,
            0.0,
        ),
        0,
    )
    windows = 2 ** (1 + levels)
    counts = jnp.minimum(query_pos[:, None] + 1, windows[None, :]).astype(jnp.float32)
    window_mean = picked / counts[:, :, None]
    grouped = pool_in.reshape(row_count, group_count, GROUP_DIM).astype(jnp.float32)
    pool_mixed = (window_mean - grouped).astype(jnp.bfloat16)
    pooled = (
        (
            jnp.einsum("tgc,gce->tge", pool_mixed, pool_map, preferred_element_type=jnp.float32)
            * pool_scale.reshape(group_count, GROUP_DIM)
        )
        .astype(jnp.bfloat16)
        .reshape(row_count, group_count * GROUP_DIM)
    )
    branches = jnp.concatenate([pooled, attn], 1)
    partial_value = jnp.dot(
        branches,
        lax.all_gather(out_local, ("sp", "fs"), axis=1, tiled=True),
        preferred_element_type=jnp.float32,
    )
    layer_out = lax.psum_scatter(
        partial_value.astype(jnp.bfloat16), "tp", scatter_dimension=1, tiled=True
    )
    return layer_out[None]


VMEM = pl.BlockSpec(memory_space=pltpu.VMEM)
SMEM = pl.BlockSpec(memory_space=pltpu.SMEM)
HBM = pl.BlockSpec(memory_space=pltpu.HBM)
VMEM_LIMIT = 24 * 1024 * 1024
WHOLE_VMEM = 60 * 1024 * 1024


def call(kernel, outs, scratch, cost, specs, *args, limit=VMEM_LIMIT):
    flops, moved, exps = cost
    return pl.pallas_call(
        kernel,
        out_shape=[jax.ShapeDtypeStruct(shape, dtype) for shape, dtype in outs],
        in_specs=specs,
        out_specs=[VMEM] * len(outs),
        scratch_shapes=scratch,
        compiler_params=pltpu.CompilerParams(vmem_limit_bytes=limit),
        cost_estimate=pl.CostEstimate(flops=flops, bytes_accessed=moved, transcendentals=exps),
    )(*args)


def move(pairs_of, outs, count, *args, limit=VMEM_LIMIT):
    def kernel(*refs):
        sems = refs[-1]
        copies = [
            pltpu.make_async_copy(source, target, sems.at[i])
            for i, (source, target) in enumerate(pairs_of(refs[: len(args)], refs[len(args) : -1]))
        ]
        for copy in copies:
            copy.start()
        for copy in copies:
            copy.wait()

    moved = sum(2 * math.prod(shape) * 2 for shape, _ in outs)
    return call(
        kernel, outs, [pltpu.SemaphoreType.DMA((count,))], (0, moved, 0), [HBM] * len(args), *args,
        limit=limit,
    )


def tiles(start, size):
    return pl.ds(pl.multiple_of(start * size, size), size)


def project_kernel(slot, *refs):
    *xs, w_ref, turn_ref, out_ref = refs if slot == 0 else refs[:-1]
    rows = out_ref.shape[0]
    if slot:
        x_ref = refs[-1]
        tp = lax.axis_index("tp")
        half = xs[0].shape[0]
        x_ref[tiles(tp, half)] = xs[0][...]
        x_ref[tiles(1 - tp, half)] = xs[1][...]
    else:
        x_ref = xs[0]
    width = w_ref.shape[1] // 4
    table = turn_ref[tiles(lax.axis_index("sp") ^ slot, rows)]
    other = pltpu.roll(table, HEAD_DIM // 2, 1)
    front = lax.broadcasted_iota(jnp.int32, table.shape, 1) < HEAD_DIM // 2
    cosine, sine = jnp.where(front, table, other), jnp.where(front, -other, table)
    for part in range(4):
        product = jnp.dot(
            x_ref[...], w_ref[:, part * width : (part + 1) * width], preferred_element_type=jnp.float32
        ).astype(jnp.bfloat16)
        if part in (1, 2):
            raw = product.astype(jnp.float32)
            turned = [
                raw[:, m : m + HEAD_DIM] * cosine
                + pltpu.roll(raw[:, m : m + HEAD_DIM], HEAD_DIM // 2, 1) * sine
                for m in range(0, width, HEAD_DIM)
            ]
            product = jnp.concatenate(turned, 1).astype(jnp.bfloat16)
        out_ref[:, part * width : (part + 1) * width] = product


def mix_kernel(slot, total, *refs):
    projs, (map_ref, scale_ref, gain_ref, lam_ref, w_ref, sent_ref, kept_ref, branch_ref) = (
        refs[:total],
        refs[total:],
    )
    rows = projs[0].shape[0]
    width = 2 * HEAD_DIM
    place = lax.axis_index("sp")
    group = lax.axis_index("tp") * total + place
    level = lax.rem(group, 4)
    block = place ^ slot
    scale = HEAD_DIM ** (-0.5)
    ahead = lax.broadcasted_iota(jnp.int32, (rows, rows), 0) >= lax.broadcasted_iota(
        jnp.int32, (rows, rows), 1
    )
    halves = []
    for m in range(2):
        begin = GROUP_DIM + m * HEAD_DIM
        query = projs[slot][:, begin : begin + HEAD_DIM]
        scores, tops = [], []
        for j in range(total):
            score = lax.dot_general(
                query,
                projs[j][:, begin + width : begin + width + HEAD_DIM],
                (((1,), (1,)), ((), ())),
                preferred_element_type=jnp.float32,
            )
            if j == slot:
                score = jnp.where(ahead, score, -jnp.inf)
                tops.append(jnp.max(score, -1, keepdims=True))
            else:
                bias = jnp.where((place ^ j) < block, 0.0, -jnp.inf)
                tops.append(jnp.max(score, -1, keepdims=True) + bias)
            scores.append(score)
        largest = functools.reduce(jnp.maximum, tops)
        sums, summed = 0.0, 0.0
        for j in range(total):
            limit = largest
            if j != slot:
                limit = largest + jnp.where((place ^ j) < block, 0.0, jnp.inf)
            expons = jnp.exp((scores[j] - limit) * scale)
            sums = sums + jnp.sum(expons, -1, keepdims=True)
            summed = summed + jnp.dot(
                expons.astype(jnp.bfloat16),
                projs[j][:, GROUP_DIM + 2 * width :],
                preferred_element_type=jnp.float32,
            )
        halves.append(summed / sums)
    raw = halves[0] - lam_ref[group] * halves[1]
    attn = (
        raw
        * lax.rsqrt(jnp.mean(raw * raw, -1, keepdims=True) + HEAD_EPS)
        * gain_ref[...]
        * HEAD_SCALE
    ).astype(jnp.bfloat16)
    branch_ref[:, GROUP_DIM:] = attn

    reach = 16
    rim = jnp.zeros((reach, GROUP_DIM), jnp.bfloat16)
    for j in range(total):
        rim = jnp.where((place ^ j) == block - 1, projs[j][rows - reach :, :GROUP_DIM], rim)
    flat = jnp.concatenate([rim, projs[slot][:, :GROUP_DIM]], 0).astype(jnp.float32)
    sums = flat
    picked = jnp.zeros((rows, GROUP_DIM), jnp.float32)
    for power in range(4):
        sums = sums + pltpu.roll(sums, 2**power, 0)
        picked = jnp.where(level == power, sums[reach:], picked)
    window = lax.shift_left(jnp.int32(2), level)
    own_pos = block * rows + lax.broadcasted_iota(jnp.int32, (rows, GROUP_DIM), 0)
    counts = jnp.minimum(own_pos + 1, window).astype(jnp.float32)
    mixed = (picked / counts - flat[reach:]).astype(jnp.bfloat16)
    pooled = jnp.dot(mixed, map_ref[place], preferred_element_type=jnp.float32) * scale_ref[pl.ds(place, 1)]
    branch_ref[:, :GROUP_DIM] = pooled.astype(jnp.bfloat16)
    sent_ref[...] = jnp.dot(
        branch_ref[...], w_ref[1], preferred_element_type=jnp.float32
    ).astype(jnp.bfloat16)
    kept_ref[...] = jnp.dot(branch_ref[...], w_ref[0], preferred_element_type=jnp.float32)


def swap(value, axis, bits):
    return lax.ppermute(value, axis, [(i, i ^ bits) for i in range(lax.axis_size(axis))])


def after(value, *earlier):
    return lax.optimization_barrier((value, *earlier))[0]


def square(front, back):
    back_one, front_two = swap(back, "fs", 1), swap(front, "fs", 2)
    front_one, back_two = swap(front, "fs", 1), swap(back, "fs", 2)
    front_three = swap(front_two, "fs", 1)
    back_three = swap(back_one, "fs", 2)
    return [(front, back), (front_one, back_one), (front_two, back_two), (front_three, back_three)]


def spread(
    tokens,
    norm_gain,
    pool_input,
    query_weight,
    key_weight,
    value_weight,
    pool_map,
    pool_scale,
    head_gain,
    diff_lambda,
    out_pool,
    out_heads,
):
    low, wide = jnp.bfloat16, jnp.float32
    n_sp, n_fs, n_tp = (lax.axis_size(axis) for axis in ("sp", "fs", "tp"))
    tp = lax.axis_index("tp")
    rows, depth = tokens.shape[1:]
    shard = depth // (n_sp * n_fs)
    channels = GROUP_DIM + 2 * HEAD_DIM
    width = GROUP_DIM + 3 * 2 * HEAD_DIM
    part = width // 4

    def columns(sources, targets):
        sp = lax.axis_index("sp")
        return [
            (source.at[:, tiles(sp ^ j, part)], targets[j].at[:, i * part : (i + 1) * part])
            for j in (*range(n_sp - 1, 0, -1), 0)
            for i, source in enumerate(sources)
        ]

    pieces = move(
        columns, [((shard, width), low)] * n_sp, 4 * n_sp,
        pool_input, query_weight, key_weight, value_weight, limit=WHOLE_VMEM,
    )
    near = [pieces[0]] + [swap(pieces[0], "fs", i) for i in range(1, n_fs)]
    far = [swap(pieces[j], "sp", j) for j in range(1, n_sp)]
    half_shard = shard // 2

    def bundle(sources, targets):
        return [
            (source.at[tiles(side, half_shard)], targets[side].at[tiles(i, half_shard)])
            for side in range(2)
            for i, source in enumerate(sources)
        ]

    bundled = move(bundle, [(((n_sp - 1) * half_shard, width), low)] * 2, 2 * (n_sp - 1), *far)
    distant = [part for pair in square(*bundled) for part in pair]

    def assemble(sources, targets):
        sp, fs = lax.axis_index("sp"), lax.axis_index("fs")
        pairs = []
        for i in range(n_fs):
            pairs.append((sources[i], targets[0].at[tiles(sp * n_fs + (fs ^ i), shard)]))
            for j in range(1, n_sp):
                place = (sp ^ j) * n_fs + (fs ^ i)
                for side in range(2):
                    source = sources[n_fs + 2 * i + side].at[tiles(j - 1, half_shard)]
                    pairs.append((source, targets[0].at[tiles(2 * place + side, half_shard)]))
        return pairs

    (weight,) = move(assemble, [((depth, width), low)], n_fs * (2 * n_sp - 1), *near, *distant)

    size = channels // 2

    def rows_of(sources, targets):
        sp = lax.axis_index("sp")
        return [
            (source.at[tiles(sp ^ j, size)], targets[j].at[tiles(i, size)])
            for j in range(n_sp)
            for i, source in enumerate(sources)
        ]

    pieces_out = move(
        rows_of, [((channels, shard), low)] * n_sp, 2 * n_sp, out_pool, out_heads,
        limit=WHOLE_VMEM,
    )
    far_out = [pieces_out[0]] + [swap(pieces_out[j], "sp", j) for j in range(1, n_sp)]

    def bundle_out(sources, targets):
        return [
            (source.at[tiles(side, size)], targets[side].at[tiles(j, size)])
            for side in range(2)
            for j, source in enumerate(sources)
        ]

    bundled_out = move(bundle_out, [((n_sp * size, shard), low)] * 2, 2 * n_sp, *far_out)

    def assemble_out(sources, targets):
        sp, fs, tp = (lax.axis_index(axis) for axis in ("sp", "fs", "tp"))
        per = n_sp // n_tp
        pairs = []
        for i in range(n_fs):
            for j in range(n_sp):
                other = sp ^ j
                here = tiles(lax.rem(other, per) * n_fs + (fs ^ i), shard)
                target = targets[0].at[lax.div(other, per) ^ tp]
                for side in range(2):
                    source = sources[2 * i + side].at[tiles(j, size)]
                    pairs.append((source, target.at[tiles(side, size), here]))
        return pairs

    (out_weight,) = move(
        assemble_out, [((n_tp, channels, depth // n_tp), low)], 2 * n_sp * n_fs,
        *[part for pair in square(*bundled_out) for part in pair],
    )

    floated = tokens[0].astype(wide)
    own = (
        floated * lax.rsqrt(jnp.mean(floated * floated, -1, keepdims=True) + NORM_EPS) * norm_gain
    ).astype(low)
    half = rows // n_tp
    mine = lax.dynamic_slice_in_dim(own, tp * half, half, 0)
    slots = {0: mine}
    for bit in (2, 1):
        for j in sorted(slots, reverse=True):
            slots[j ^ bit] = swap(slots[j], "sp", bit)

    half_dim = HEAD_DIM // 2
    freqs = 1.0 / THETA ** (np.arange(half_dim, dtype=np.float32) * 2.0 / HEAD_DIM)
    angles = np.arange(rows * n_sp, dtype=np.float64)[:, None] * freqs[None, :]
    table = jnp.asarray(np.concatenate([np.cos(angles), np.sin(angles)], 1).astype(np.float32))

    def project(j):
        xs = [own] if j == 0 else [slots[j], swap(slots[j], "tp", 1)]
        scratch = [pltpu.VMEM((rows, depth), low)] if j else []
        return call(
            functools.partial(project_kernel, j), [((rows, width), low)], scratch,
            (2 * rows * depth * width, 2 * depth * width, 0), [VMEM] * (len(xs) + 2),
            *xs, weight, table,
        )[0]

    projs = [project(j) for j in range(n_sp)]
    gain = head_gain[None]

    def block_sum(slot, gain):
        sent, kept = call(
            functools.partial(mix_kernel, slot, n_sp),
            [((rows, depth // n_tp), low), ((rows, depth // n_tp), wide)],
            [pltpu.VMEM((rows, channels), low)],
            (8 * rows * rows * n_sp * HEAD_DIM + 2 * rows * channels * depth, 8 * rows * width + 2 * depth * channels,
             2 * rows * rows * n_sp),
            [VMEM] * (n_sp + 3) + [SMEM, VMEM],
            *projs, pool_map, pool_scale.reshape(n_sp, GROUP_DIM), gain, diff_lambda, out_weight,
        )
        return kept + swap(sent, "tp", 1).astype(wide)

    sum_three = block_sum(3, gain).astype(low)
    from_three = swap(sum_three, "sp", 1)
    gain = after(gain, sum_three)
    sum_two = (block_sum(2, gain) + from_three.astype(wide)).astype(low)
    sum_one = after(block_sum(1, gain).astype(low), from_three)
    from_two = swap(sum_two, "sp", 2)
    from_one = swap(sum_one, "sp", 1)
    result = block_sum(0, gain) + from_one.astype(wide) + from_two.astype(wide)
    return result.astype(low)[None]


def solution(mesh):
    placed = (
        P("fs", "sp", None),
        P(),
        P(("sp", "fs"), "tp"),
        P(("sp", "fs"), "tp"),
        P(("sp", "fs"), "tp"),
        P(("sp", "fs"), "tp"),
        P("tp", None, None),
        P("tp"),
        P(),
        P(),
        P("tp", ("sp", "fs")),
        P("tp", ("sp", "fs")),
    )

    def body(*args):
        n_sp, n_fs, n_tp = (mesh.shape[axis] for axis in ("sp", "fs", "tp"))
        groups, heads = args[6].shape[0], args[5].shape[1] // (2 * HEAD_DIM)
        pairs = groups == heads == n_sp == n_fs == 4 and n_tp == 2
        return (spread if pairs else local)(*args)

    return jax.shard_map(
        body, mesh=mesh, in_specs=placed, out_specs=P("fs", "sp", "tp"), check_vma=False
    )
```

```python
import functools
import math

import jax
import jax.numpy as jnp
import numpy as np
from jax import lax
from jax.experimental import pallas as pl
from jax.experimental.pallas import tpu as pltpu
from jax.sharding import PartitionSpec as P


HEAD_DIM = 128
GROUP_DIM = 256


THETA = 500000.0
HEAD_SCALE = 0.8
NORM_EPS = 1e-06
HEAD_EPS = 1e-05


def from_behind(value, axis, steps):
    count = lax.axis_size(axis)
    first, last = (max(0, -steps), min(count, count - steps))
    return lax.ppermute(value, axis, [(source, source + steps) for source in range(first, last)])


def rotate(tensor, positions):
    half = HEAD_DIM // 2
    freqs = 1.0 / THETA ** (jnp.arange(half, dtype=jnp.float32) * 2.0 / HEAD_DIM)
    angles = positions[:, None] * freqs[None, :]
    cosine = jnp.cos(angles)[:, None, None, :]
    sine = jnp.sin(angles)[:, None, None, :]
    floated = tensor.astype(jnp.float32)
    first = floated[..., :half]
    second = floated[..., half:]
    turned = jnp.concatenate([first * cosine - second * sine, second * cosine + first * sine], -1)
    return turned.astype(jnp.bfloat16)


def local(
    tokens,
    norm_gain,
    pool_input,
    query_weight,
    key_weight,
    value_weight,
    pool_map,
    pool_scale,
    head_gain,
    diff_lambda,
    out_pool,
    out_heads,
):
    out_local = jnp.concatenate([out_pool, out_heads], 0)
    row_count = tokens.shape[1]
    floated = tokens[0].astype(jnp.float32)
    normed = (
        floated * lax.rsqrt(jnp.mean(floated * floated, -1, keepdims=True) + NORM_EPS) * norm_gain
    ).astype(jnp.bfloat16)
    fragments = (
        lax.all_gather(pool_input, ("sp", "fs"), axis=0, tiled=True),
        lax.all_gather(query_weight, ("sp", "fs"), axis=0, tiled=True),
        lax.all_gather(key_weight, ("sp", "fs"), axis=0, tiled=True),
        lax.all_gather(value_weight, ("sp", "fs"), axis=0, tiled=True),
    )
    projected = tuple(
        (jnp.dot(normed, fragment, preferred_element_type=jnp.float32) for fragment in fragments)
    )
    pool_in, queries, keys_flat, values_flat = [
        product.astype(jnp.bfloat16) for product in projected
    ]
    head_count = values_flat.shape[1] // (2 * HEAD_DIM)
    tp_index = lax.axis_index("tp")
    sp_index = lax.axis_index("sp")
    query_pos = sp_index * row_count + jnp.arange(row_count, dtype=jnp.int32)
    positions = query_pos.astype(jnp.float32)
    queries = rotate(queries.reshape(row_count, head_count, 2, HEAD_DIM), positions)
    keys_flat = rotate(keys_flat.reshape(row_count, head_count, 2, HEAD_DIM), positions).reshape(
        row_count, head_count * 2 * HEAD_DIM
    )
    lambdas = lax.dynamic_slice_in_dim(diff_lambda, tp_index * head_count, head_count, 0)

    def online_step(state, key_rows, value_rows, key_offset):
        largest, summed, accum = state
        width = key_rows.shape[0]
        shaped = key_rows.reshape(width, head_count, 2, HEAD_DIM)
        scores = jnp.einsum(
            "qhcd,khcd->chqk", queries, shaped, preferred_element_type=jnp.float32
        ) * HEAD_DIM ** (-0.5)
        key_pos = key_offset + jnp.arange(width, dtype=jnp.int32)
        scores = jnp.where(query_pos[:, None] >= key_pos[None, :], scores, -jnp.inf)
        newest = jnp.maximum(largest, jnp.max(scores, -1))
        anchor = jnp.where(jnp.isfinite(newest), newest, 0.0)
        rescale = jnp.exp(largest - anchor)
        expons = jnp.exp(scores - anchor[..., None])
        summed = summed * rescale + jnp.sum(expons, -1)
        value_shaped = value_rows.reshape(width, head_count, 2 * HEAD_DIM)
        added = jnp.einsum(
            "chqk,khe->chqe",
            expons.astype(jnp.bfloat16),
            value_shaped,
            preferred_element_type=jnp.float32,
        )
        accum = accum * rescale[..., None] + added
        return (newest, summed, accum)

    start_state = (
        jnp.full((2, head_count, row_count), -jnp.inf, jnp.float32),
        jnp.zeros((2, head_count, row_count), jnp.float32),
        jnp.zeros((2, head_count, row_count, 2 * HEAD_DIM), jnp.float32),
    )
    fragments = (
        lax.all_gather(keys_flat, "sp", axis=0, tiled=True),
        lax.all_gather(values_flat, "sp", axis=0, tiled=True),
    )
    span = math.gcd(fragments[0].shape[0], 1024)

    def inner_step(index, inner_state):
        key_rows = lax.dynamic_slice_in_dim(fragments[0], index * span, span, 0)
        value_rows = lax.dynamic_slice_in_dim(fragments[1], index * span, span, 0)
        return online_step(inner_state, key_rows, value_rows, index * span)

    final_state = lax.fori_loop(0, fragments[0].shape[0] // span, inner_step, start_state)
    summed_final = final_state[1]
    accum_final = final_state[2]
    heads_raw = (
        accum_final[0] / summed_final[0][..., None]
        - lambdas[:, None, None] * accum_final[1] / summed_final[1][..., None]
    )
    heads_raw = jnp.moveaxis(heads_raw, 0, 1)
    attn = (
        (
            heads_raw
            * lax.rsqrt(jnp.mean(heads_raw * heads_raw, -1, keepdims=True) + HEAD_EPS)
            * head_gain
            * HEAD_SCALE
        )
        .astype(jnp.bfloat16)
        .reshape(row_count, head_count * 2 * HEAD_DIM)
    )
    reach = 15
    rim_rows = from_behind(pool_in[row_count - reach :], "sp", 1)
    extended = jnp.concatenate([rim_rows, pool_in], 0).astype(jnp.float32)
    pair_sums = extended[1:] + extended[:-1]
    quad_sums = pair_sums[2:] + pair_sums[:-2]
    octet_sums = quad_sums[4:] + quad_sums[:-4]
    sixteen_sums = octet_sums[8:] + octet_sums[:-8]
    group_count = pool_in.shape[1] // GROUP_DIM
    stacked = jnp.stack(
        [
            pair_sums[14 : 14 + row_count],
            quad_sums[12 : 12 + row_count],
            octet_sums[8 : 8 + row_count],
            sixteen_sums,
        ],
        0,
    ).reshape(4, row_count, group_count, GROUP_DIM)
    levels = (tp_index * group_count + jnp.arange(group_count, dtype=jnp.int32)) % 4
    picked = jnp.sum(
        jnp.where(
            levels[None, None, :, None] == jnp.arange(4, dtype=jnp.int32)[:, None, None, None],
            stacked,
            0.0,
        ),
        0,
    )
    windows = 2 ** (1 + levels)
    counts = jnp.minimum(query_pos[:, None] + 1, windows[None, :]).astype(jnp.float32)
    window_mean = picked / counts[:, :, None]
    grouped = pool_in.reshape(row_count, group_count, GROUP_DIM).astype(jnp.float32)
    pool_mixed = (window_mean - grouped).astype(jnp.bfloat16)
    pooled = (
        (
            jnp.einsum("tgc,gce->tge", pool_mixed, pool_map, preferred_element_type=jnp.float32)
            * pool_scale.reshape(group_count, GROUP_DIM)
        )
        .astype(jnp.bfloat16)
        .reshape(row_count, group_count * GROUP_DIM)
    )
    branches = jnp.concatenate([pooled, attn], 1)
    partial_value = jnp.dot(
        branches,
        lax.all_gather(out_local, ("sp", "fs"), axis=1, tiled=True),
        preferred_element_type=jnp.float32,
    )
    layer_out = lax.psum_scatter(
        partial_value.astype(jnp.bfloat16), "tp", scatter_dimension=1, tiled=True
    )
    return layer_out[None]


VMEM = pl.BlockSpec(memory_space=pltpu.VMEM)
SMEM = pl.BlockSpec(memory_space=pltpu.SMEM)
HBM = pl.BlockSpec(memory_space=pltpu.HBM)
VMEM_LIMIT = 16 * 1024 * 1024
WHOLE_VMEM = 60 * 1024 * 1024


def call(kernel, outs, scratch, cost, specs, *args, limit=VMEM_LIMIT):
    flops, moved, exps = cost
    return pl.pallas_call(
        kernel,
        out_shape=[jax.ShapeDtypeStruct(shape, dtype) for shape, dtype in outs],
        in_specs=specs,
        out_specs=[VMEM] * len(outs),
        scratch_shapes=scratch,
        compiler_params=pltpu.CompilerParams(vmem_limit_bytes=limit),
        cost_estimate=pl.CostEstimate(flops=flops, bytes_accessed=moved, transcendentals=exps),
    )(*args)


def move(pairs_of, outs, count, *args, limit=VMEM_LIMIT):
    def kernel(*refs):
        sems = refs[-1]
        copies = [
            pltpu.make_async_copy(source, target, sems.at[i])
            for i, (source, target) in enumerate(pairs_of(refs[: len(args)], refs[len(args) : -1]))
        ]
        for copy in copies:
            copy.start()
        for copy in copies:
            copy.wait()

    moved = sum(2 * math.prod(shape) * 2 for shape, _ in outs)
    return call(
        kernel, outs, [pltpu.SemaphoreType.DMA((count,))], (0, moved, 0), [HBM] * len(args), *args,
        limit=limit,
    )


def place(pairs_of, outs, *args):
    def kernel(*refs):
        for source, target in pairs_of(refs[: len(args)], refs[len(args) :]):
            target[...] = source[...]

    moved = sum(2 * math.prod(shape) * 2 for shape, _ in outs)
    return call(kernel, outs, [], (0, moved, 0), [VMEM] * len(args), *args)


def tiles(start, size):
    return pl.ds(pl.multiple_of(start * size, size), size)


def project_kernel(slot, *refs):
    *xs, w_ref, turn_ref, out_ref = refs if slot == 0 else refs[:-1]
    rows = out_ref.shape[0]
    if slot:
        x_ref = refs[-1]
        tp = lax.axis_index("tp")
        half = xs[0].shape[0]
        x_ref[tiles(tp, half)] = xs[0][...]
        x_ref[tiles(1 - tp, half)] = xs[1][...]
    else:
        x_ref = xs[0]
    width = w_ref.shape[1] // 4
    table = turn_ref[tiles(lax.axis_index("sp") ^ slot, rows)]
    other = pltpu.roll(table, HEAD_DIM // 2, 1)
    front = lax.broadcasted_iota(jnp.int32, table.shape, 1) < HEAD_DIM // 2
    cosine, sine = jnp.where(front, table, other), jnp.where(front, -other, table)
    for part in range(4):
        product = jnp.dot(
            x_ref[...], w_ref[:, part * width : (part + 1) * width], preferred_element_type=jnp.float32
        ).astype(jnp.bfloat16)
        if part in (1, 2):
            raw = product.astype(jnp.float32)
            turned = [
                raw[:, m : m + HEAD_DIM] * cosine
                + pltpu.roll(raw[:, m : m + HEAD_DIM], HEAD_DIM // 2, 1) * sine
                for m in range(0, width, HEAD_DIM)
            ]
            product = jnp.concatenate(turned, 1).astype(jnp.bfloat16)
        out_ref[:, part * width : (part + 1) * width] = product


def mix_kernel(slot, total, *refs):
    projs, (map_ref, scale_ref, gain_ref, lam_ref, w_ref, sent_ref, kept_ref, branch_ref) = (
        refs[:total],
        refs[total:],
    )
    rows = projs[0].shape[0]
    width = 2 * HEAD_DIM
    place = lax.axis_index("sp")
    group = lax.axis_index("tp") * total + place
    level = lax.rem(group, 4)
    block = place ^ slot
    scale = HEAD_DIM ** (-0.5)
    ahead = lax.broadcasted_iota(jnp.int32, (rows, rows), 0) >= lax.broadcasted_iota(
        jnp.int32, (rows, rows), 1
    )
    halves = []
    for m in range(2):
        begin = GROUP_DIM + m * HEAD_DIM
        query = projs[slot][:, begin : begin + HEAD_DIM]
        scores, tops = [], []
        for j in range(total):
            score = lax.dot_general(
                query,
                projs[j][:, begin + width : begin + width + HEAD_DIM],
                (((1,), (1,)), ((), ())),
                preferred_element_type=jnp.float32,
            )
            if j == slot:
                score = jnp.where(ahead, score, -jnp.inf)
                tops.append(jnp.max(score, -1, keepdims=True))
            else:
                bias = jnp.where((place ^ j) < block, 0.0, -jnp.inf)
                tops.append(jnp.max(score, -1, keepdims=True) + bias)
            scores.append(score)
        largest = functools.reduce(jnp.maximum, tops)
        sums, summed = 0.0, 0.0
        for j in range(total):
            limit = largest
            if j != slot:
                limit = largest + jnp.where((place ^ j) < block, 0.0, jnp.inf)
            expons = jnp.exp((scores[j] - limit) * scale)
            sums = sums + jnp.sum(expons, -1, keepdims=True)
            summed = summed + jnp.dot(
                expons.astype(jnp.bfloat16),
                projs[j][:, GROUP_DIM + 2 * width :],
                preferred_element_type=jnp.float32,
            )
        halves.append(summed / sums)
    raw = halves[0] - lam_ref[group] * halves[1]
    attn = (
        raw
        * lax.rsqrt(jnp.mean(raw * raw, -1, keepdims=True) + HEAD_EPS)
        * gain_ref[...]
        * HEAD_SCALE
    ).astype(jnp.bfloat16)
    branch_ref[:, GROUP_DIM:] = attn

    reach = 16
    rim = jnp.zeros((reach, GROUP_DIM), jnp.bfloat16)
    for j in range(total):
        rim = jnp.where((place ^ j) == block - 1, projs[j][rows - reach :, :GROUP_DIM], rim)
    flat = jnp.concatenate([rim, projs[slot][:, :GROUP_DIM]], 0).astype(jnp.float32)
    sums = flat
    picked = jnp.zeros((rows, GROUP_DIM), jnp.float32)
    for power in range(4):
        sums = sums + pltpu.roll(sums, 2**power, 0)
        picked = jnp.where(level == power, sums[reach:], picked)
    window = lax.shift_left(jnp.int32(2), level)
    own_pos = block * rows + lax.broadcasted_iota(jnp.int32, (rows, GROUP_DIM), 0)
    counts = jnp.minimum(own_pos + 1, window).astype(jnp.float32)
    mixed = (picked / counts - flat[reach:]).astype(jnp.bfloat16)
    pooled = jnp.dot(mixed, map_ref[place], preferred_element_type=jnp.float32) * scale_ref[:, tiles(place, GROUP_DIM)]
    branch_ref[:, :GROUP_DIM] = pooled.astype(jnp.bfloat16)
    sent_ref[...] = jnp.dot(
        branch_ref[...], w_ref[1], preferred_element_type=jnp.float32
    ).astype(jnp.bfloat16)
    kept_ref[...] = jnp.dot(branch_ref[...], w_ref[0], preferred_element_type=jnp.float32)


def swap(value, axis, bits):
    return lax.ppermute(value, axis, [(i, i ^ bits) for i in range(lax.axis_size(axis))])


def after(value, *earlier):
    return lax.optimization_barrier((value, *earlier))[0]


def square(front, back):
    back_one, front_two = swap(back, "fs", 1), swap(front, "fs", 2)
    front_one, back_two = swap(front, "fs", 1), swap(back, "fs", 2)
    front_three = swap(front_two, "fs", 1)
    back_three = swap(back_one, "fs", 2)
    return [(front, back), (front_one, back_one), (front_two, back_two), (front_three, back_three)]


def spread(
    tokens,
    norm_gain,
    pool_input,
    query_weight,
    key_weight,
    value_weight,
    pool_map,
    pool_scale,
    head_gain,
    diff_lambda,
    out_pool,
    out_heads,
):
    low, wide = jnp.bfloat16, jnp.float32
    n_sp, n_fs, n_tp = (lax.axis_size(axis) for axis in ("sp", "fs", "tp"))
    tp = lax.axis_index("tp")
    rows, depth = tokens.shape[1:]
    shard = depth // (n_sp * n_fs)
    channels = GROUP_DIM + 2 * HEAD_DIM
    width = GROUP_DIM + 3 * 2 * HEAD_DIM
    part = width // 4

    def columns(sources, targets):
        sp = lax.axis_index("sp")
        return [
            (source.at[:, tiles(sp ^ j, part)], targets[j].at[:, i * part : (i + 1) * part])
            for j in (*range(n_sp - 1, 0, -1), 0)
            for i, source in enumerate(sources)
        ]

    pieces = move(
        columns, [((shard, width), low)] * n_sp, 4 * n_sp,
        pool_input, query_weight, key_weight, value_weight, limit=WHOLE_VMEM,
    )
    near = [pieces[0]] + [swap(pieces[0], "fs", i) for i in range(1, n_fs)]
    far = [swap(pieces[j], "sp", j) for j in range(1, n_sp)]
    half_shard = shard // 2

    def bundle(sources, targets):
        return [
            (source.at[tiles(side, half_shard)], targets[side].at[tiles(i, half_shard)])
            for side in range(2)
            for i, source in enumerate(sources)
        ]

    bundled = place(bundle, [(((n_sp - 1) * half_shard, width), low)] * 2, *far)
    distant = [part for pair in square(*bundled) for part in pair]

    def assemble(sources, targets):
        sp, fs = lax.axis_index("sp"), lax.axis_index("fs")
        pairs = []
        for i in range(n_fs):
            pairs.append((sources[i], targets[0].at[tiles(sp * n_fs + (fs ^ i), shard)]))
            for j in range(1, n_sp):
                place = (sp ^ j) * n_fs + (fs ^ i)
                for side in range(2):
                    source = sources[n_fs + 2 * i + side].at[tiles(j - 1, half_shard)]
                    pairs.append((source, targets[0].at[tiles(2 * place + side, half_shard)]))
        return pairs

    (weight,) = place(assemble, [((depth, width), low)], *near, *distant)

    size = channels // 2

    def rows_of(sources, targets):
        sp = lax.axis_index("sp")
        return [
            (source.at[tiles(sp ^ j, size)], targets[j].at[tiles(i, size)])
            for j in range(n_sp)
            for i, source in enumerate(sources)
        ]

    pieces_out = move(
        rows_of, [((channels, shard), low)] * n_sp, 2 * n_sp, out_pool, out_heads,
        limit=WHOLE_VMEM,
    )
    far_out = [pieces_out[0]] + [swap(pieces_out[j], "sp", j) for j in range(1, n_sp)]

    def bundle_out(sources, targets):
        return [
            (source.at[tiles(side, size)], targets[side].at[tiles(j, size)])
            for side in range(2)
            for j, source in enumerate(sources)
        ]

    bundled_out = place(bundle_out, [((n_sp * size, shard), low)] * 2, *far_out)

    def assemble_out(sources, targets):
        sp, fs, tp = (lax.axis_index(axis) for axis in ("sp", "fs", "tp"))
        per = n_sp // n_tp
        pairs = []
        for i in range(n_fs):
            for j in range(n_sp):
                other = sp ^ j
                here = tiles(lax.rem(other, per) * n_fs + (fs ^ i), shard)
                target = targets[0].at[lax.div(other, per) ^ tp]
                for side in range(2):
                    source = sources[2 * i + side].at[tiles(j, size)]
                    pairs.append((source, target.at[tiles(side, size), here]))
        return pairs

    (out_weight,) = place(
        assemble_out, [((n_tp, channels, depth // n_tp), low)],
        *[part for pair in square(*bundled_out) for part in pair],
    )

    floated = tokens[0].astype(wide)
    own = (
        floated * lax.rsqrt(jnp.mean(floated * floated, -1, keepdims=True) + NORM_EPS) * norm_gain
    ).astype(low)
    half = rows // n_tp
    mine = lax.dynamic_slice_in_dim(own, tp * half, half, 0)
    slots = {0: mine}
    for bit in (2, 1):
        for j in sorted(slots, reverse=True):
            slots[j ^ bit] = swap(slots[j], "sp", bit)

    half_dim = HEAD_DIM // 2
    freqs = 1.0 / THETA ** (np.arange(half_dim, dtype=np.float32) * 2.0 / HEAD_DIM)
    angles = np.arange(rows * n_sp, dtype=np.float64)[:, None] * freqs[None, :]
    table = jnp.asarray(np.concatenate([np.cos(angles), np.sin(angles)], 1).astype(np.float32))

    def project(j):
        xs = [own] if j == 0 else [slots[j], swap(slots[j], "tp", 1)]
        scratch = [pltpu.VMEM((rows, depth), low)] if j else []
        return call(
            functools.partial(project_kernel, j), [((rows, width), low)], scratch,
            (2 * rows * depth * width, 2 * depth * width, 0), [VMEM] * (len(xs) + 2),
            *xs, weight, table,
        )[0]

    projs = [project(j) for j in range(n_sp)]
    gain = head_gain[None]

    def block_sum(slot, gain):
        sent, kept = call(
            functools.partial(mix_kernel, slot, n_sp),
            [((rows, depth // n_tp), low), ((rows, depth // n_tp), wide)],
            [pltpu.VMEM((rows, channels), low)],
            (8 * rows * rows * n_sp * HEAD_DIM + 2 * rows * channels * depth, 8 * rows * width + 2 * depth * channels,
             2 * rows * rows * n_sp),
            [VMEM] * (n_sp + 3) + [SMEM, VMEM],
            *projs, pool_map, pool_scale[None], gain, diff_lambda, out_weight,
        )
        return kept + swap(sent, "tp", 1).astype(wide)

    sum_three = block_sum(3, gain).astype(low)
    from_three = swap(sum_three, "sp", 1)
    gain = after(gain, sum_three)
    sum_two = (block_sum(2, gain) + from_three.astype(wide)).astype(low)
    sum_one = after(block_sum(1, gain).astype(low), from_three)
    from_two = swap(sum_two, "sp", 2)
    from_one = swap(sum_one, "sp", 1)
    result = block_sum(0, gain) + from_one.astype(wide) + from_two.astype(wide)
    return result.astype(low)[None]


def solution(mesh):
    placed = (
        P("fs", "sp", None),
        P(),
        P(("sp", "fs"), "tp"),
        P(("sp", "fs"), "tp"),
        P(("sp", "fs"), "tp"),
        P(("sp", "fs"), "tp"),
        P("tp", None, None),
        P("tp"),
        P(),
        P(),
        P("tp", ("sp", "fs")),
        P("tp", ("sp", "fs")),
    )

    def body(*args):
        n_sp, n_fs, n_tp = (mesh.shape[axis] for axis in ("sp", "fs", "tp"))
        groups, heads = args[6].shape[0], args[5].shape[1] // (2 * HEAD_DIM)
        pairs = groups == heads == n_sp == n_fs == 4 and n_tp == 2
        return (spread if pairs else local)(*args)

    return jax.shard_map(
        body, mesh=mesh, in_specs=placed, out_specs=P("fs", "sp", "tp"), check_vma=False
    )
```

```python
import functools
import math

import jax
import jax.numpy as jnp
import numpy as np
from jax import lax
from jax.experimental import pallas as pl
from jax.experimental.pallas import tpu as pltpu
from jax.sharding import PartitionSpec as P


HEAD_DIM = 128
GROUP_DIM = 256


THETA = 500000.0
HEAD_SCALE = 0.8
NORM_EPS = 1e-06
HEAD_EPS = 1e-05


def from_behind(value, axis, steps):
    count = lax.axis_size(axis)
    first, last = (max(0, -steps), min(count, count - steps))
    return lax.ppermute(value, axis, [(source, source + steps) for source in range(first, last)])


def rotate(tensor, positions):
    half = HEAD_DIM // 2
    freqs = 1.0 / THETA ** (jnp.arange(half, dtype=jnp.float32) * 2.0 / HEAD_DIM)
    angles = positions[:, None] * freqs[None, :]
    cosine = jnp.cos(angles)[:, None, None, :]
    sine = jnp.sin(angles)[:, None, None, :]
    floated = tensor.astype(jnp.float32)
    first = floated[..., :half]
    second = floated[..., half:]
    turned = jnp.concatenate([first * cosine - second * sine, second * cosine + first * sine], -1)
    return turned.astype(jnp.bfloat16)


def local(
    tokens,
    norm_gain,
    pool_input,
    query_weight,
    key_weight,
    value_weight,
    pool_map,
    pool_scale,
    head_gain,
    diff_lambda,
    out_pool,
    out_heads,
):
    out_local = jnp.concatenate([out_pool, out_heads], 0)
    row_count = tokens.shape[1]
    floated = tokens[0].astype(jnp.float32)
    normed = (
        floated * lax.rsqrt(jnp.mean(floated * floated, -1, keepdims=True) + NORM_EPS) * norm_gain
    ).astype(jnp.bfloat16)
    fragments = (
        lax.all_gather(pool_input, ("sp", "fs"), axis=0, tiled=True),
        lax.all_gather(query_weight, ("sp", "fs"), axis=0, tiled=True),
        lax.all_gather(key_weight, ("sp", "fs"), axis=0, tiled=True),
        lax.all_gather(value_weight, ("sp", "fs"), axis=0, tiled=True),
    )
    projected = tuple(
        (jnp.dot(normed, fragment, preferred_element_type=jnp.float32) for fragment in fragments)
    )
    pool_in, queries, keys_flat, values_flat = [
        product.astype(jnp.bfloat16) for product in projected
    ]
    head_count = values_flat.shape[1] // (2 * HEAD_DIM)
    tp_index = lax.axis_index("tp")
    sp_index = lax.axis_index("sp")
    query_pos = sp_index * row_count + jnp.arange(row_count, dtype=jnp.int32)
    positions = query_pos.astype(jnp.float32)
    queries = rotate(queries.reshape(row_count, head_count, 2, HEAD_DIM), positions)
    keys_flat = rotate(keys_flat.reshape(row_count, head_count, 2, HEAD_DIM), positions).reshape(
        row_count, head_count * 2 * HEAD_DIM
    )
    lambdas = lax.dynamic_slice_in_dim(diff_lambda, tp_index * head_count, head_count, 0)

    def online_step(state, key_rows, value_rows, key_offset):
        largest, summed, accum = state
        width = key_rows.shape[0]
        shaped = key_rows.reshape(width, head_count, 2, HEAD_DIM)
        scores = jnp.einsum(
            "qhcd,khcd->chqk", queries, shaped, preferred_element_type=jnp.float32
        ) * HEAD_DIM ** (-0.5)
        key_pos = key_offset + jnp.arange(width, dtype=jnp.int32)
        scores = jnp.where(query_pos[:, None] >= key_pos[None, :], scores, -jnp.inf)
        newest = jnp.maximum(largest, jnp.max(scores, -1))
        anchor = jnp.where(jnp.isfinite(newest), newest, 0.0)
        rescale = jnp.exp(largest - anchor)
        expons = jnp.exp(scores - anchor[..., None])
        summed = summed * rescale + jnp.sum(expons, -1)
        value_shaped = value_rows.reshape(width, head_count, 2 * HEAD_DIM)
        added = jnp.einsum(
            "chqk,khe->chqe",
            expons.astype(jnp.bfloat16),
            value_shaped,
            preferred_element_type=jnp.float32,
        )
        accum = accum * rescale[..., None] + added
        return (newest, summed, accum)

    start_state = (
        jnp.full((2, head_count, row_count), -jnp.inf, jnp.float32),
        jnp.zeros((2, head_count, row_count), jnp.float32),
        jnp.zeros((2, head_count, row_count, 2 * HEAD_DIM), jnp.float32),
    )
    fragments = (
        lax.all_gather(keys_flat, "sp", axis=0, tiled=True),
        lax.all_gather(values_flat, "sp", axis=0, tiled=True),
    )
    span = math.gcd(fragments[0].shape[0], 1024)

    def inner_step(index, inner_state):
        key_rows = lax.dynamic_slice_in_dim(fragments[0], index * span, span, 0)
        value_rows = lax.dynamic_slice_in_dim(fragments[1], index * span, span, 0)
        return online_step(inner_state, key_rows, value_rows, index * span)

    final_state = lax.fori_loop(0, fragments[0].shape[0] // span, inner_step, start_state)
    summed_final = final_state[1]
    accum_final = final_state[2]
    heads_raw = (
        accum_final[0] / summed_final[0][..., None]
        - lambdas[:, None, None] * accum_final[1] / summed_final[1][..., None]
    )
    heads_raw = jnp.moveaxis(heads_raw, 0, 1)
    attn = (
        (
            heads_raw
            * lax.rsqrt(jnp.mean(heads_raw * heads_raw, -1, keepdims=True) + HEAD_EPS)
            * head_gain
            * HEAD_SCALE
        )
        .astype(jnp.bfloat16)
        .reshape(row_count, head_count * 2 * HEAD_DIM)
    )
    reach = 15
    rim_rows = from_behind(pool_in[row_count - reach :], "sp", 1)
    extended = jnp.concatenate([rim_rows, pool_in], 0).astype(jnp.float32)
    pair_sums = extended[1:] + extended[:-1]
    quad_sums = pair_sums[2:] + pair_sums[:-2]
    octet_sums = quad_sums[4:] + quad_sums[:-4]
    sixteen_sums = octet_sums[8:] + octet_sums[:-8]
    group_count = pool_in.shape[1] // GROUP_DIM
    stacked = jnp.stack(
        [
            pair_sums[14 : 14 + row_count],
            quad_sums[12 : 12 + row_count],
            octet_sums[8 : 8 + row_count],
            sixteen_sums,
        ],
        0,
    ).reshape(4, row_count, group_count, GROUP_DIM)
    levels = (tp_index * group_count + jnp.arange(group_count, dtype=jnp.int32)) % 4
    picked = jnp.sum(
        jnp.where(
            levels[None, None, :, None] == jnp.arange(4, dtype=jnp.int32)[:, None, None, None],
            stacked,
            0.0,
        ),
        0,
    )
    windows = 2 ** (1 + levels)
    counts = jnp.minimum(query_pos[:, None] + 1, windows[None, :]).astype(jnp.float32)
    window_mean = picked / counts[:, :, None]
    grouped = pool_in.reshape(row_count, group_count, GROUP_DIM).astype(jnp.float32)
    pool_mixed = (window_mean - grouped).astype(jnp.bfloat16)
    pooled = (
        (
            jnp.einsum("tgc,gce->tge", pool_mixed, pool_map, preferred_element_type=jnp.float32)
            * pool_scale.reshape(group_count, GROUP_DIM)
        )
        .astype(jnp.bfloat16)
        .reshape(row_count, group_count * GROUP_DIM)
    )
    branches = jnp.concatenate([pooled, attn], 1)
    partial_value = jnp.dot(
        branches,
        lax.all_gather(out_local, ("sp", "fs"), axis=1, tiled=True),
        preferred_element_type=jnp.float32,
    )
    layer_out = lax.psum_scatter(
        partial_value.astype(jnp.bfloat16), "tp", scatter_dimension=1, tiled=True
    )
    return layer_out[None]


VMEM = pl.BlockSpec(memory_space=pltpu.VMEM)
SMEM = pl.BlockSpec(memory_space=pltpu.SMEM)
HBM = pl.BlockSpec(memory_space=pltpu.HBM)
CHUNKS = 2
VMEM_LIMIT = 16 * 1024 * 1024
WHOLE_VMEM = 60 * 1024 * 1024


def call(kernel, outs, scratch, cost, specs, *args, limit=VMEM_LIMIT):
    flops, moved, exps = cost
    return pl.pallas_call(
        kernel,
        out_shape=[jax.ShapeDtypeStruct(shape, dtype) for shape, dtype in outs],
        in_specs=specs,
        out_specs=[VMEM] * len(outs),
        scratch_shapes=scratch,
        compiler_params=pltpu.CompilerParams(vmem_limit_bytes=limit),
        cost_estimate=pl.CostEstimate(flops=flops, bytes_accessed=moved, transcendentals=exps),
    )(*args)


def move(pairs_of, outs, count, *args, limit=VMEM_LIMIT):
    def kernel(*refs):
        sems = refs[-1]
        copies = [
            pltpu.make_async_copy(source, target, sems.at[i])
            for i, (source, target) in enumerate(pairs_of(refs[: len(args)], refs[len(args) : -1]))
        ]
        for copy in copies:
            copy.start()
        for copy in copies:
            copy.wait()

    moved = sum(2 * math.prod(shape) * 2 for shape, _ in outs)
    return call(
        kernel, outs, [pltpu.SemaphoreType.DMA((count,))], (0, moved, 0), [HBM] * len(args), *args,
        limit=limit,
    )


def place(pairs_of, outs, *args):
    def kernel(*refs):
        for source, target in pairs_of(refs[: len(args)], refs[len(args) :]):
            target[...] = source[...]

    moved = sum(2 * math.prod(shape) * 2 for shape, _ in outs)
    return call(kernel, outs, [], (0, moved, 0), [VMEM] * len(args), *args)


def tiles(start, size):
    return pl.ds(pl.multiple_of(start * size, size), size)


def project_kernel(slot, *refs):
    *xs, w_ref, turn_ref, out_ref = refs if slot == 0 else refs[:-1]
    rows = out_ref.shape[0]
    if slot:
        x_ref = refs[-1]
        tp = lax.axis_index("tp")
        size = xs[0].shape[0]
        each = len(xs) // 2
        for c in range(each):
            x_ref[tiles(tp * each + c, size)] = xs[c][...]
            x_ref[tiles((1 - tp) * each + c, size)] = xs[each + c][...]
    else:
        x_ref = xs[0]
    width = w_ref.shape[1] // 4
    table = turn_ref[tiles(lax.axis_index("sp") ^ slot, rows)]
    other = pltpu.roll(table, HEAD_DIM // 2, 1)
    front = lax.broadcasted_iota(jnp.int32, table.shape, 1) < HEAD_DIM // 2
    cosine, sine = jnp.where(front, table, other), jnp.where(front, -other, table)
    for part in range(4):
        product = jnp.dot(
            x_ref[...], w_ref[:, part * width : (part + 1) * width], preferred_element_type=jnp.float32
        ).astype(jnp.bfloat16)
        if part in (1, 2):
            raw = product.astype(jnp.float32)
            turned = [
                raw[:, m : m + HEAD_DIM] * cosine
                + pltpu.roll(raw[:, m : m + HEAD_DIM], HEAD_DIM // 2, 1) * sine
                for m in range(0, width, HEAD_DIM)
            ]
            product = jnp.concatenate(turned, 1).astype(jnp.bfloat16)
        out_ref[:, part * width : (part + 1) * width] = product


def mix_kernel(slot, total, *refs):
    projs, (map_ref, scale_ref, gain_ref, lam_ref, w_ref, sent_ref, kept_ref, branch_ref) = (
        refs[:total],
        refs[total:],
    )
    rows = projs[0].shape[0]
    width = 2 * HEAD_DIM
    place = lax.axis_index("sp")
    group = lax.axis_index("tp") * total + place
    level = lax.rem(group, 4)
    block = place ^ slot
    scale = HEAD_DIM ** (-0.5)
    ahead = lax.broadcasted_iota(jnp.int32, (rows, rows), 0) >= lax.broadcasted_iota(
        jnp.int32, (rows, rows), 1
    )
    halves = []
    for m in range(2):
        begin = GROUP_DIM + m * HEAD_DIM
        query = projs[slot][:, begin : begin + HEAD_DIM]
        scores, tops = [], []
        for j in range(total):
            score = lax.dot_general(
                query,
                projs[j][:, begin + width : begin + width + HEAD_DIM],
                (((1,), (1,)), ((), ())),
                preferred_element_type=jnp.float32,
            )
            if j == slot:
                score = jnp.where(ahead, score, -jnp.inf)
                tops.append(jnp.max(score, -1, keepdims=True))
            else:
                bias = jnp.where((place ^ j) < block, 0.0, -jnp.inf)
                tops.append(jnp.max(score, -1, keepdims=True) + bias)
            scores.append(score)
        largest = functools.reduce(jnp.maximum, tops)
        sums, summed = 0.0, 0.0
        for j in range(total):
            limit = largest
            if j != slot:
                limit = largest + jnp.where((place ^ j) < block, 0.0, jnp.inf)
            expons = jnp.exp((scores[j] - limit) * scale)
            sums = sums + jnp.sum(expons, -1, keepdims=True)
            summed = summed + jnp.dot(
                expons.astype(jnp.bfloat16),
                projs[j][:, GROUP_DIM + 2 * width :],
                preferred_element_type=jnp.float32,
            )
        halves.append(summed / sums)
    raw = halves[0] - lam_ref[group] * halves[1]
    attn = (
        raw
        * lax.rsqrt(jnp.mean(raw * raw, -1, keepdims=True) + HEAD_EPS)
        * gain_ref[...]
        * HEAD_SCALE
    ).astype(jnp.bfloat16)
    branch_ref[:, GROUP_DIM:] = attn

    reach = 16
    rim = jnp.zeros((reach, GROUP_DIM), jnp.bfloat16)
    for j in range(total):
        rim = jnp.where((place ^ j) == block - 1, projs[j][rows - reach :, :GROUP_DIM], rim)
    flat = jnp.concatenate([rim, projs[slot][:, :GROUP_DIM]], 0).astype(jnp.float32)
    sums = flat
    picked = jnp.zeros((rows, GROUP_DIM), jnp.float32)
    for power in range(4):
        sums = sums + pltpu.roll(sums, 2**power, 0)
        picked = jnp.where(level == power, sums[reach:], picked)
    window = lax.shift_left(jnp.int32(2), level)
    own_pos = block * rows + lax.broadcasted_iota(jnp.int32, (rows, GROUP_DIM), 0)
    counts = jnp.minimum(own_pos + 1, window).astype(jnp.float32)
    mixed = (picked / counts - flat[reach:]).astype(jnp.bfloat16)
    pooled = jnp.dot(mixed, map_ref[place], preferred_element_type=jnp.float32) * scale_ref[:, tiles(place, GROUP_DIM)]
    branch_ref[:, :GROUP_DIM] = pooled.astype(jnp.bfloat16)
    sent_ref[...] = jnp.dot(
        branch_ref[...], w_ref[1], preferred_element_type=jnp.float32
    ).astype(jnp.bfloat16)
    kept_ref[...] = jnp.dot(branch_ref[...], w_ref[0], preferred_element_type=jnp.float32)


def swap(value, axis, bits):
    return lax.ppermute(value, axis, [(i, i ^ bits) for i in range(lax.axis_size(axis))])


def after(value, *earlier):
    return lax.optimization_barrier((value, *earlier))[0]


def square(front, back):
    back_one, front_two = swap(back, "fs", 1), swap(front, "fs", 2)
    front_one, back_two = swap(front, "fs", 1), swap(back, "fs", 2)
    front_three = swap(front_two, "fs", 1)
    back_three = swap(back_one, "fs", 2)
    return [(front, back), (front_one, back_one), (front_two, back_two), (front_three, back_three)]


def spread(
    tokens,
    norm_gain,
    pool_input,
    query_weight,
    key_weight,
    value_weight,
    pool_map,
    pool_scale,
    head_gain,
    diff_lambda,
    out_pool,
    out_heads,
):
    low, wide = jnp.bfloat16, jnp.float32
    n_sp, n_fs, n_tp = (lax.axis_size(axis) for axis in ("sp", "fs", "tp"))
    tp = lax.axis_index("tp")
    rows, depth = tokens.shape[1:]
    shard = depth // (n_sp * n_fs)
    channels = GROUP_DIM + 2 * HEAD_DIM
    width = GROUP_DIM + 3 * 2 * HEAD_DIM
    part = width // 4

    def columns(sources, targets):
        sp = lax.axis_index("sp")
        return [
            (source.at[:, tiles(sp ^ j, part)], targets[j].at[:, i * part : (i + 1) * part])
            for j in (*range(n_sp - 1, 0, -1), 0)
            for i, source in enumerate(sources)
        ]

    pieces = move(
        columns, [((shard, width), low)] * n_sp, 4 * n_sp,
        pool_input, query_weight, key_weight, value_weight, limit=WHOLE_VMEM,
    )
    near = [pieces[0]] + [swap(pieces[0], "fs", i) for i in range(1, n_fs)]
    far = [swap(pieces[j], "sp", j) for j in range(1, n_sp)]
    half_shard = shard // 2

    def bundle(sources, targets):
        return [
            (source.at[tiles(side, half_shard)], targets[side].at[tiles(i, half_shard)])
            for side in range(2)
            for i, source in enumerate(sources)
        ]

    bundled = place(bundle, [(((n_sp - 1) * half_shard, width), low)] * 2, *far)
    distant = [part for pair in square(*bundled) for part in pair]

    def assemble(sources, targets):
        sp, fs = lax.axis_index("sp"), lax.axis_index("fs")
        pairs = []
        for i in range(n_fs):
            pairs.append((sources[i], targets[0].at[tiles(sp * n_fs + (fs ^ i), shard)]))
            for j in range(1, n_sp):
                place = (sp ^ j) * n_fs + (fs ^ i)
                for side in range(2):
                    source = sources[n_fs + 2 * i + side].at[tiles(j - 1, half_shard)]
                    pairs.append((source, targets[0].at[tiles(2 * place + side, half_shard)]))
        return pairs

    (weight,) = place(assemble, [((depth, width), low)], *near, *distant)

    size = channels // 2

    def rows_of(sources, targets):
        sp = lax.axis_index("sp")
        return [
            (source.at[tiles(sp ^ j, size)], targets[j].at[tiles(i, size)])
            for j in range(n_sp)
            for i, source in enumerate(sources)
        ]

    pieces_out = move(
        rows_of, [((channels, shard), low)] * n_sp, 2 * n_sp, out_pool, out_heads,
        limit=WHOLE_VMEM,
    )
    far_out = [pieces_out[0]] + [swap(pieces_out[j], "sp", j) for j in range(1, n_sp)]

    def bundle_out(sources, targets):
        return [
            (source.at[tiles(side, size)], targets[side].at[tiles(j, size)])
            for side in range(2)
            for j, source in enumerate(sources)
        ]

    bundled_out = place(bundle_out, [((n_sp * size, shard), low)] * 2, *far_out)

    def assemble_out(sources, targets):
        sp, fs, tp = (lax.axis_index(axis) for axis in ("sp", "fs", "tp"))
        per = n_sp // n_tp
        pairs = []
        for i in range(n_fs):
            for j in range(n_sp):
                other = sp ^ j
                here = tiles(lax.rem(other, per) * n_fs + (fs ^ i), shard)
                target = targets[0].at[lax.div(other, per) ^ tp]
                for side in range(2):
                    source = sources[2 * i + side].at[tiles(j, size)]
                    pairs.append((source, target.at[tiles(side, size), here]))
        return pairs

    (out_weight,) = place(
        assemble_out, [((n_tp, channels, depth // n_tp), low)],
        *[part for pair in square(*bundled_out) for part in pair],
    )

    floated = tokens[0].astype(wide)
    own = (
        floated * lax.rsqrt(jnp.mean(floated * floated, -1, keepdims=True) + NORM_EPS) * norm_gain
    ).astype(low)
    half = rows // n_tp
    size_of = half // CHUNKS
    mine = [
        lax.dynamic_slice_in_dim(own, tp * half + c * size_of, size_of, 0) for c in range(CHUNKS)
    ]
    whole = lax.dynamic_slice_in_dim(own, tp * half, half, 0)
    slots = {1: [swap(whole, "sp", 1)]}
    slots[2] = [swap(piece, "sp", 2) for piece in mine]
    slots[3] = [swap(piece, "sp", 1) for piece in slots[2]]

    half_dim = HEAD_DIM // 2
    freqs = 1.0 / THETA ** (np.arange(half_dim, dtype=np.float32) * 2.0 / HEAD_DIM)
    angles = np.arange(rows * n_sp, dtype=np.float64)[:, None] * freqs[None, :]
    table = jnp.asarray(np.concatenate([np.cos(angles), np.sin(angles)], 1).astype(np.float32))

    def project(j):
        xs = [own]
        if j:
            xs = slots[j] + [swap(piece, "tp", 1) for piece in slots[j]]
        scratch = [pltpu.VMEM((rows, depth), low)] if j else []
        return call(
            functools.partial(project_kernel, j), [((rows, width), low)], scratch,
            (2 * rows * depth * width, 2 * depth * width, 0), [VMEM] * (len(xs) + 2),
            *xs, weight, table,
        )[0]

    projs = [project(j) for j in range(n_sp)]
    gain = head_gain[None]

    def block_sum(slot, gain):
        sent, kept = call(
            functools.partial(mix_kernel, slot, n_sp),
            [((rows, depth // n_tp), low), ((rows, depth // n_tp), wide)],
            [pltpu.VMEM((rows, channels), low)],
            (8 * rows * rows * n_sp * HEAD_DIM + 2 * rows * channels * depth, 8 * rows * width + 2 * depth * channels,
             2 * rows * rows * n_sp),
            [VMEM] * (n_sp + 3) + [SMEM, VMEM],
            *projs, pool_map, pool_scale[None], gain, diff_lambda, out_weight,
        )
        return kept + swap(sent, "tp", 1).astype(wide)

    sum_three = block_sum(3, gain).astype(low)
    from_three = swap(sum_three, "sp", 1)
    gain = after(gain, sum_three)
    sum_two = (block_sum(2, gain) + from_three.astype(wide)).astype(low)
    sum_one = after(block_sum(1, gain).astype(low), from_three)
    from_two = swap(sum_two, "sp", 2)
    from_one = swap(sum_one, "sp", 1)
    result = block_sum(0, gain) + from_one.astype(wide) + from_two.astype(wide)
    return result.astype(low)[None]


def solution(mesh):
    placed = (
        P("fs", "sp", None),
        P(),
        P(("sp", "fs"), "tp"),
        P(("sp", "fs"), "tp"),
        P(("sp", "fs"), "tp"),
        P(("sp", "fs"), "tp"),
        P("tp", None, None),
        P("tp"),
        P(),
        P(),
        P("tp", ("sp", "fs")),
        P("tp", ("sp", "fs")),
    )

    def body(*args):
        n_sp, n_fs, n_tp = (mesh.shape[axis] for axis in ("sp", "fs", "tp"))
        groups, heads = args[6].shape[0], args[5].shape[1] // (2 * HEAD_DIM)
        pairs = groups == heads == n_sp == n_fs == 4 and n_tp == 2
        return (spread if pairs else local)(*args)

    return jax.shard_map(
        body, mesh=mesh, in_specs=placed, out_specs=P("fs", "sp", "tp"), check_vma=False
    )
```

```python
import functools
import math

import jax
import jax.numpy as jnp
import numpy as np
from jax import lax
from jax.experimental import pallas as pl
from jax.experimental.pallas import tpu as pltpu
from jax.sharding import PartitionSpec as P


HEAD_DIM = 128
GROUP_DIM = 256


THETA = 500000.0
HEAD_SCALE = 0.8
NORM_EPS = 1e-06
HEAD_EPS = 1e-05


def from_behind(value, axis, steps):
    count = lax.axis_size(axis)
    first, last = (max(0, -steps), min(count, count - steps))
    return lax.ppermute(value, axis, [(source, source + steps) for source in range(first, last)])


def rotate(tensor, positions):
    half = HEAD_DIM // 2
    freqs = 1.0 / THETA ** (jnp.arange(half, dtype=jnp.float32) * 2.0 / HEAD_DIM)
    angles = positions[:, None] * freqs[None, :]
    cosine = jnp.cos(angles)[:, None, None, :]
    sine = jnp.sin(angles)[:, None, None, :]
    floated = tensor.astype(jnp.float32)
    first = floated[..., :half]
    second = floated[..., half:]
    turned = jnp.concatenate([first * cosine - second * sine, second * cosine + first * sine], -1)
    return turned.astype(jnp.bfloat16)


def local(
    tokens,
    norm_gain,
    pool_input,
    query_weight,
    key_weight,
    value_weight,
    pool_map,
    pool_scale,
    head_gain,
    diff_lambda,
    out_pool,
    out_heads,
):
    out_local = jnp.concatenate([out_pool, out_heads], 0)
    row_count = tokens.shape[1]
    floated = tokens[0].astype(jnp.float32)
    normed = (
        floated * lax.rsqrt(jnp.mean(floated * floated, -1, keepdims=True) + NORM_EPS) * norm_gain
    ).astype(jnp.bfloat16)
    fragments = (
        lax.all_gather(pool_input, ("sp", "fs"), axis=0, tiled=True),
        lax.all_gather(query_weight, ("sp", "fs"), axis=0, tiled=True),
        lax.all_gather(key_weight, ("sp", "fs"), axis=0, tiled=True),
        lax.all_gather(value_weight, ("sp", "fs"), axis=0, tiled=True),
    )
    projected = tuple(
        (jnp.dot(normed, fragment, preferred_element_type=jnp.float32) for fragment in fragments)
    )
    pool_in, queries, keys_flat, values_flat = [
        product.astype(jnp.bfloat16) for product in projected
    ]
    head_count = values_flat.shape[1] // (2 * HEAD_DIM)
    tp_index = lax.axis_index("tp")
    sp_index = lax.axis_index("sp")
    query_pos = sp_index * row_count + jnp.arange(row_count, dtype=jnp.int32)
    positions = query_pos.astype(jnp.float32)
    queries = rotate(queries.reshape(row_count, head_count, 2, HEAD_DIM), positions)
    keys_flat = rotate(keys_flat.reshape(row_count, head_count, 2, HEAD_DIM), positions).reshape(
        row_count, head_count * 2 * HEAD_DIM
    )
    lambdas = lax.dynamic_slice_in_dim(diff_lambda, tp_index * head_count, head_count, 0)

    def online_step(state, key_rows, value_rows, key_offset):
        largest, summed, accum = state
        width = key_rows.shape[0]
        shaped = key_rows.reshape(width, head_count, 2, HEAD_DIM)
        scores = jnp.einsum(
            "qhcd,khcd->chqk", queries, shaped, preferred_element_type=jnp.float32
        ) * HEAD_DIM ** (-0.5)
        key_pos = key_offset + jnp.arange(width, dtype=jnp.int32)
        scores = jnp.where(query_pos[:, None] >= key_pos[None, :], scores, -jnp.inf)
        newest = jnp.maximum(largest, jnp.max(scores, -1))
        anchor = jnp.where(jnp.isfinite(newest), newest, 0.0)
        rescale = jnp.exp(largest - anchor)
        expons = jnp.exp(scores - anchor[..., None])
        summed = summed * rescale + jnp.sum(expons, -1)
        value_shaped = value_rows.reshape(width, head_count, 2 * HEAD_DIM)
        added = jnp.einsum(
            "chqk,khe->chqe",
            expons.astype(jnp.bfloat16),
            value_shaped,
            preferred_element_type=jnp.float32,
        )
        accum = accum * rescale[..., None] + added
        return (newest, summed, accum)

    start_state = (
        jnp.full((2, head_count, row_count), -jnp.inf, jnp.float32),
        jnp.zeros((2, head_count, row_count), jnp.float32),
        jnp.zeros((2, head_count, row_count, 2 * HEAD_DIM), jnp.float32),
    )
    fragments = (
        lax.all_gather(keys_flat, "sp", axis=0, tiled=True),
        lax.all_gather(values_flat, "sp", axis=0, tiled=True),
    )
    span = math.gcd(fragments[0].shape[0], 1024)

    def inner_step(index, inner_state):
        key_rows = lax.dynamic_slice_in_dim(fragments[0], index * span, span, 0)
        value_rows = lax.dynamic_slice_in_dim(fragments[1], index * span, span, 0)
        return online_step(inner_state, key_rows, value_rows, index * span)

    final_state = lax.fori_loop(0, fragments[0].shape[0] // span, inner_step, start_state)
    summed_final = final_state[1]
    accum_final = final_state[2]
    heads_raw = (
        accum_final[0] / summed_final[0][..., None]
        - lambdas[:, None, None] * accum_final[1] / summed_final[1][..., None]
    )
    heads_raw = jnp.moveaxis(heads_raw, 0, 1)
    attn = (
        (
            heads_raw
            * lax.rsqrt(jnp.mean(heads_raw * heads_raw, -1, keepdims=True) + HEAD_EPS)
            * head_gain
            * HEAD_SCALE
        )
        .astype(jnp.bfloat16)
        .reshape(row_count, head_count * 2 * HEAD_DIM)
    )
    reach = 15
    rim_rows = from_behind(pool_in[row_count - reach :], "sp", 1)
    extended = jnp.concatenate([rim_rows, pool_in], 0).astype(jnp.float32)
    pair_sums = extended[1:] + extended[:-1]
    quad_sums = pair_sums[2:] + pair_sums[:-2]
    octet_sums = quad_sums[4:] + quad_sums[:-4]
    sixteen_sums = octet_sums[8:] + octet_sums[:-8]
    group_count = pool_in.shape[1] // GROUP_DIM
    stacked = jnp.stack(
        [
            pair_sums[14 : 14 + row_count],
            quad_sums[12 : 12 + row_count],
            octet_sums[8 : 8 + row_count],
            sixteen_sums,
        ],
        0,
    ).reshape(4, row_count, group_count, GROUP_DIM)
    levels = (tp_index * group_count + jnp.arange(group_count, dtype=jnp.int32)) % 4
    picked = jnp.sum(
        jnp.where(
            levels[None, None, :, None] == jnp.arange(4, dtype=jnp.int32)[:, None, None, None],
            stacked,
            0.0,
        ),
        0,
    )
    windows = 2 ** (1 + levels)
    counts = jnp.minimum(query_pos[:, None] + 1, windows[None, :]).astype(jnp.float32)
    window_mean = picked / counts[:, :, None]
    grouped = pool_in.reshape(row_count, group_count, GROUP_DIM).astype(jnp.float32)
    pool_mixed = (window_mean - grouped).astype(jnp.bfloat16)
    pooled = (
        (
            jnp.einsum("tgc,gce->tge", pool_mixed, pool_map, preferred_element_type=jnp.float32)
            * pool_scale.reshape(group_count, GROUP_DIM)
        )
        .astype(jnp.bfloat16)
        .reshape(row_count, group_count * GROUP_DIM)
    )
    branches = jnp.concatenate([pooled, attn], 1)
    partial_value = jnp.dot(
        branches,
        lax.all_gather(out_local, ("sp", "fs"), axis=1, tiled=True),
        preferred_element_type=jnp.float32,
    )
    layer_out = lax.psum_scatter(
        partial_value.astype(jnp.bfloat16), "tp", scatter_dimension=1, tiled=True
    )
    return layer_out[None]


VMEM = pl.BlockSpec(memory_space=pltpu.VMEM)
SMEM = pl.BlockSpec(memory_space=pltpu.SMEM)
HBM = pl.BlockSpec(memory_space=pltpu.HBM)
CHUNKS = 2
VMEM_LIMIT = 16 * 1024 * 1024
WHOLE_VMEM = 60 * 1024 * 1024


def call(kernel, outs, scratch, cost, specs, *args, limit=VMEM_LIMIT):
    flops, moved, exps = cost
    return pl.pallas_call(
        kernel,
        out_shape=[jax.ShapeDtypeStruct(shape, dtype) for shape, dtype in outs],
        in_specs=specs,
        out_specs=[VMEM] * len(outs),
        scratch_shapes=scratch,
        compiler_params=pltpu.CompilerParams(vmem_limit_bytes=limit),
        cost_estimate=pl.CostEstimate(flops=flops, bytes_accessed=moved, transcendentals=exps),
    )(*args)


def move(pairs_of, outs, count, *args, limit=VMEM_LIMIT):
    def kernel(*refs):
        sems = refs[-1]
        copies = [
            pltpu.make_async_copy(source, target, sems.at[i])
            for i, (source, target) in enumerate(pairs_of(refs[: len(args)], refs[len(args) : -1]))
        ]
        for copy in copies:
            copy.start()
        for copy in copies:
            copy.wait()

    moved = sum(2 * math.prod(shape) * 2 for shape, _ in outs)
    return call(
        kernel, outs, [pltpu.SemaphoreType.DMA((count,))], (0, moved, 0), [HBM] * len(args), *args,
        limit=limit,
    )


def place(pairs_of, outs, *args):
    def kernel(*refs):
        for source, target in pairs_of(refs[: len(args)], refs[len(args) :]):
            target[...] = source[...]

    moved = sum(2 * math.prod(shape) * 2 for shape, _ in outs)
    return call(kernel, outs, [], (0, moved, 0), [VMEM] * len(args), *args)


def tiles(start, size):
    return pl.ds(pl.multiple_of(start * size, size), size)


def project_kernel(slot, *refs):
    *xs, w_ref, turn_ref, out_ref = refs if slot == 0 else refs[:-1]
    rows = out_ref.shape[0]
    if slot:
        x_ref = refs[-1]
        tp = lax.axis_index("tp")
        size = xs[0].shape[0]
        each = len(xs) // 2
        for c in range(each):
            x_ref[tiles(tp * each + c, size)] = xs[c][...]
            x_ref[tiles((1 - tp) * each + c, size)] = xs[each + c][...]
    else:
        x_ref = xs[0]
    width = w_ref.shape[1] // 4
    table = turn_ref[tiles(lax.axis_index("sp") ^ slot, rows)]
    other = pltpu.roll(table, HEAD_DIM // 2, 1)
    front = lax.broadcasted_iota(jnp.int32, table.shape, 1) < HEAD_DIM // 2
    cosine, sine = jnp.where(front, table, other), jnp.where(front, -other, table)
    for part in range(4):
        product = jnp.dot(
            x_ref[...], w_ref[:, part * width : (part + 1) * width], preferred_element_type=jnp.float32
        ).astype(jnp.bfloat16)
        if part in (1, 2):
            raw = product.astype(jnp.float32)
            turned = [
                raw[:, m : m + HEAD_DIM] * cosine
                + pltpu.roll(raw[:, m : m + HEAD_DIM], HEAD_DIM // 2, 1) * sine
                for m in range(0, width, HEAD_DIM)
            ]
            product = jnp.concatenate(turned, 1).astype(jnp.bfloat16)
        out_ref[:, part * width : (part + 1) * width] = product


def mix_kernel(slot, total, part, parts, *refs):
    projs, (map_ref, scale_ref, gain_ref, lam_ref, w_ref, sent_ref, kept_ref, branch_ref) = (
        refs[:total],
        refs[total:],
    )
    rows = projs[0].shape[0]
    size = rows // parts
    first = part * size
    mine = slice(first, first + size)
    width = 2 * HEAD_DIM
    place = lax.axis_index("sp")
    group = lax.axis_index("tp") * total + place
    level = lax.rem(group, 4)
    block = place ^ slot
    scale = HEAD_DIM ** (-0.5)
    ahead = lax.broadcasted_iota(jnp.int32, (size, rows), 0) + first >= lax.broadcasted_iota(
        jnp.int32, (size, rows), 1
    )
    halves = []
    for m in range(2):
        begin = GROUP_DIM + m * HEAD_DIM
        query = projs[slot][mine, begin : begin + HEAD_DIM]
        scores, tops = [], []
        for j in range(total):
            score = lax.dot_general(
                query,
                projs[j][:, begin + width : begin + width + HEAD_DIM],
                (((1,), (1,)), ((), ())),
                preferred_element_type=jnp.float32,
            )
            if j == slot:
                score = jnp.where(ahead, score, -jnp.inf)
                tops.append(jnp.max(score, -1, keepdims=True))
            else:
                bias = jnp.where((place ^ j) < block, 0.0, -jnp.inf)
                tops.append(jnp.max(score, -1, keepdims=True) + bias)
            scores.append(score)
        largest = functools.reduce(jnp.maximum, tops)
        sums, summed = 0.0, 0.0
        for j in range(total):
            limit = largest
            if j != slot:
                limit = largest + jnp.where((place ^ j) < block, 0.0, jnp.inf)
            expons = jnp.exp((scores[j] - limit) * scale)
            sums = sums + jnp.sum(expons, -1, keepdims=True)
            summed = summed + jnp.dot(
                expons.astype(jnp.bfloat16),
                projs[j][:, GROUP_DIM + 2 * width :],
                preferred_element_type=jnp.float32,
            )
        halves.append(summed / sums)
    raw = halves[0] - lam_ref[group] * halves[1]
    attn = (
        raw
        * lax.rsqrt(jnp.mean(raw * raw, -1, keepdims=True) + HEAD_EPS)
        * gain_ref[...]
        * HEAD_SCALE
    ).astype(jnp.bfloat16)
    branch_ref[:, GROUP_DIM:] = attn

    reach = 16
    if first:
        rim = projs[slot][first - reach : first, :GROUP_DIM]
    else:
        rim = jnp.zeros((reach, GROUP_DIM), jnp.bfloat16)
        for j in range(total):
            rim = jnp.where((place ^ j) == block - 1, projs[j][rows - reach :, :GROUP_DIM], rim)
    flat = jnp.concatenate([rim, projs[slot][mine, :GROUP_DIM]], 0).astype(jnp.float32)
    sums = flat
    picked = jnp.zeros((size, GROUP_DIM), jnp.float32)
    for power in range(4):
        sums = sums + pltpu.roll(sums, 2**power, 0)
        picked = jnp.where(level == power, sums[reach:], picked)
    window = lax.shift_left(jnp.int32(2), level)
    own_pos = block * rows + first + lax.broadcasted_iota(jnp.int32, (size, GROUP_DIM), 0)
    counts = jnp.minimum(own_pos + 1, window).astype(jnp.float32)
    mixed = (picked / counts - flat[reach:]).astype(jnp.bfloat16)
    pooled = jnp.dot(mixed, map_ref[place], preferred_element_type=jnp.float32) * scale_ref[:, tiles(place, GROUP_DIM)]
    branch_ref[:, :GROUP_DIM] = pooled.astype(jnp.bfloat16)
    sent_ref[...] = jnp.dot(
        branch_ref[...], w_ref[1], preferred_element_type=jnp.float32
    ).astype(jnp.bfloat16)
    kept_ref[...] = jnp.dot(branch_ref[...], w_ref[0], preferred_element_type=jnp.float32)


def swap(value, axis, bits):
    return lax.ppermute(value, axis, [(i, i ^ bits) for i in range(lax.axis_size(axis))])


def after(value, *earlier):
    return lax.optimization_barrier((value, *earlier))[0]


def square(front, back):
    back_one, front_two = swap(back, "fs", 1), swap(front, "fs", 2)
    front_one, back_two = swap(front, "fs", 1), swap(back, "fs", 2)
    front_three = swap(front_two, "fs", 1)
    back_three = swap(back_one, "fs", 2)
    return [(front, back), (front_one, back_one), (front_two, back_two), (front_three, back_three)]


def spread(
    tokens,
    norm_gain,
    pool_input,
    query_weight,
    key_weight,
    value_weight,
    pool_map,
    pool_scale,
    head_gain,
    diff_lambda,
    out_pool,
    out_heads,
):
    low, wide = jnp.bfloat16, jnp.float32
    n_sp, n_fs, n_tp = (lax.axis_size(axis) for axis in ("sp", "fs", "tp"))
    tp = lax.axis_index("tp")
    rows, depth = tokens.shape[1:]
    shard = depth // (n_sp * n_fs)
    channels = GROUP_DIM + 2 * HEAD_DIM
    width = GROUP_DIM + 3 * 2 * HEAD_DIM
    part = width // 4

    def columns(sources, targets):
        sp = lax.axis_index("sp")
        return [
            (source.at[:, tiles(sp ^ j, part)], targets[j].at[:, i * part : (i + 1) * part])
            for j in (*range(n_sp - 1, 0, -1), 0)
            for i, source in enumerate(sources)
        ]

    pieces = move(
        columns, [((shard, width), low)] * n_sp, 4 * n_sp,
        pool_input, query_weight, key_weight, value_weight, limit=WHOLE_VMEM,
    )
    near = [pieces[0]] + [swap(pieces[0], "fs", i) for i in range(1, n_fs)]
    far = [swap(pieces[j], "sp", j) for j in range(1, n_sp)]
    half_shard = shard // 2

    def bundle(sources, targets):
        return [
            (source.at[tiles(side, half_shard)], targets[side].at[tiles(i, half_shard)])
            for side in range(2)
            for i, source in enumerate(sources)
        ]

    bundled = place(bundle, [(((n_sp - 1) * half_shard, width), low)] * 2, *far)
    distant = [part for pair in square(*bundled) for part in pair]

    def assemble(sources, targets):
        sp, fs = lax.axis_index("sp"), lax.axis_index("fs")
        pairs = []
        for i in range(n_fs):
            pairs.append((sources[i], targets[0].at[tiles(sp * n_fs + (fs ^ i), shard)]))
            for j in range(1, n_sp):
                place = (sp ^ j) * n_fs + (fs ^ i)
                for side in range(2):
                    source = sources[n_fs + 2 * i + side].at[tiles(j - 1, half_shard)]
                    pairs.append((source, targets[0].at[tiles(2 * place + side, half_shard)]))
        return pairs

    (weight,) = place(assemble, [((depth, width), low)], *near, *distant)

    size = channels // 2

    def rows_of(sources, targets):
        sp = lax.axis_index("sp")
        return [
            (source.at[tiles(sp ^ j, size)], targets[j].at[tiles(i, size)])
            for j in range(n_sp)
            for i, source in enumerate(sources)
        ]

    pieces_out = move(
        rows_of, [((channels, shard), low)] * n_sp, 2 * n_sp, out_pool, out_heads,
        limit=WHOLE_VMEM,
    )
    far_out = [pieces_out[0]] + [swap(pieces_out[j], "sp", j) for j in range(1, n_sp)]

    def bundle_out(sources, targets):
        return [
            (source.at[tiles(side, size)], targets[side].at[tiles(j, size)])
            for side in range(2)
            for j, source in enumerate(sources)
        ]

    bundled_out = place(bundle_out, [((n_sp * size, shard), low)] * 2, *far_out)

    def assemble_out(sources, targets):
        sp, fs, tp = (lax.axis_index(axis) for axis in ("sp", "fs", "tp"))
        per = n_sp // n_tp
        pairs = []
        for i in range(n_fs):
            for j in range(n_sp):
                other = sp ^ j
                here = tiles(lax.rem(other, per) * n_fs + (fs ^ i), shard)
                target = targets[0].at[lax.div(other, per) ^ tp]
                for side in range(2):
                    source = sources[2 * i + side].at[tiles(j, size)]
                    pairs.append((source, target.at[tiles(side, size), here]))
        return pairs

    (out_weight,) = place(
        assemble_out, [((n_tp, channels, depth // n_tp), low)],
        *[part for pair in square(*bundled_out) for part in pair],
    )

    floated = tokens[0].astype(wide)
    own = (
        floated * lax.rsqrt(jnp.mean(floated * floated, -1, keepdims=True) + NORM_EPS) * norm_gain
    ).astype(low)
    half = rows // n_tp
    size_of = half // CHUNKS
    mine = [
        lax.dynamic_slice_in_dim(own, tp * half + c * size_of, size_of, 0) for c in range(CHUNKS)
    ]
    whole = lax.dynamic_slice_in_dim(own, tp * half, half, 0)
    slots = {1: [swap(whole, "sp", 1)]}
    slots[2] = [swap(piece, "sp", 2) for piece in mine]
    slots[3] = [swap(piece, "sp", 1) for piece in slots[2]]

    half_dim = HEAD_DIM // 2
    freqs = 1.0 / THETA ** (np.arange(half_dim, dtype=np.float32) * 2.0 / HEAD_DIM)
    angles = np.arange(rows * n_sp, dtype=np.float64)[:, None] * freqs[None, :]
    table = jnp.asarray(np.concatenate([np.cos(angles), np.sin(angles)], 1).astype(np.float32))

    def project(j):
        xs = [own]
        if j:
            xs = slots[j] + [swap(piece, "tp", 1) for piece in slots[j]]
        scratch = [pltpu.VMEM((rows, depth), low)] if j else []
        return call(
            functools.partial(project_kernel, j), [((rows, width), low)], scratch,
            (2 * rows * depth * width, 2 * depth * width, 0), [VMEM] * (len(xs) + 2),
            *xs, weight, table,
        )[0]

    projs = [project(j) for j in range(n_sp)]
    gain = head_gain[None]

    def mixed(slot, gain, part=0, parts=1):
        size = rows // parts
        sent, kept = call(
            functools.partial(mix_kernel, slot, n_sp, part, parts),
            [((size, depth // n_tp), low), ((size, depth // n_tp), wide)],
            [pltpu.VMEM((size, channels), low)],
            (8 * size * rows * n_sp * HEAD_DIM + 2 * size * channels * depth, 8 * rows * width + 2 * depth * channels,
             2 * size * rows * n_sp),
            [VMEM] * (n_sp + 3) + [SMEM, VMEM],
            *projs, pool_map, pool_scale[None], gain, diff_lambda, out_weight,
        )
        return kept, swap(sent, "tp", 1)

    def total(parts, c=None, *more):
        if c is not None:
            parts = [part[c * half : (c + 1) * half] for part in parts]
        return sum(part.astype(wide) for part in (*parts, *more))

    early = mixed(3, gain, 0, 2)
    late = mixed(3, after(gain, early[0]), 1, 2)
    sum_three = total(early).astype(low)
    from_three = [swap(sum_three, "sp", 1)]
    gain = after(gain, late[0], sum_three)
    two = mixed(2, gain)
    from_three.append(swap(after(total(late).astype(low), two[0]), "sp", 1))
    one = mixed(1, gain)
    sum_two = [total(two, 0, from_three[0]).astype(low)]
    sum_two.append(total(two, 1, after(from_three[1], sum_two[0])).astype(low))
    from_two = [swap(sum_two[c], "sp", 2) for c in range(2)]
    zero = mixed(0, gain)
    from_one = swap(total(one).astype(low), "sp", 1)
    result = [total((*zero, from_one), c, from_two[c]).astype(low) for c in range(2)]
    return jnp.concatenate(result, 0)[None]


def solution(mesh):
    placed = (
        P("fs", "sp", None),
        P(),
        P(("sp", "fs"), "tp"),
        P(("sp", "fs"), "tp"),
        P(("sp", "fs"), "tp"),
        P(("sp", "fs"), "tp"),
        P("tp", None, None),
        P("tp"),
        P(),
        P(),
        P("tp", ("sp", "fs")),
        P("tp", ("sp", "fs")),
    )

    def body(*args):
        n_sp, n_fs, n_tp = (mesh.shape[axis] for axis in ("sp", "fs", "tp"))
        groups, heads = args[6].shape[0], args[5].shape[1] // (2 * HEAD_DIM)
        pairs = groups == heads == n_sp == n_fs == 4 and n_tp == 2
        return (spread if pairs else local)(*args)

    return jax.shard_map(
        body, mesh=mesh, in_specs=placed, out_specs=P("fs", "sp", "tp"), check_vma=False
    )
```

```python
import functools
import math

import jax
import jax.numpy as jnp
import numpy as np
from jax import lax
from jax.experimental import pallas as pl
from jax.experimental.pallas import tpu as pltpu
from jax.sharding import PartitionSpec as P


HEAD_DIM = 128
GROUP_DIM = 256


THETA = 500000.0
HEAD_SCALE = 0.8
NORM_EPS = 1e-06
HEAD_EPS = 1e-05


def from_behind(value, axis, steps):
    count = lax.axis_size(axis)
    first, last = (max(0, -steps), min(count, count - steps))
    return lax.ppermute(value, axis, [(source, source + steps) for source in range(first, last)])


def rotate(tensor, positions):
    half = HEAD_DIM // 2
    freqs = 1.0 / THETA ** (jnp.arange(half, dtype=jnp.float32) * 2.0 / HEAD_DIM)
    angles = positions[:, None] * freqs[None, :]
    cosine = jnp.cos(angles)[:, None, None, :]
    sine = jnp.sin(angles)[:, None, None, :]
    floated = tensor.astype(jnp.float32)
    first = floated[..., :half]
    second = floated[..., half:]
    turned = jnp.concatenate([first * cosine - second * sine, second * cosine + first * sine], -1)
    return turned.astype(jnp.bfloat16)


def local(
    tokens,
    norm_gain,
    pool_input,
    query_weight,
    key_weight,
    value_weight,
    pool_map,
    pool_scale,
    head_gain,
    diff_lambda,
    out_pool,
    out_heads,
):
    out_local = jnp.concatenate([out_pool, out_heads], 0)
    row_count = tokens.shape[1]
    floated = tokens[0].astype(jnp.float32)
    normed = (
        floated * lax.rsqrt(jnp.mean(floated * floated, -1, keepdims=True) + NORM_EPS) * norm_gain
    ).astype(jnp.bfloat16)
    fragments = (
        lax.all_gather(pool_input, ("sp", "fs"), axis=0, tiled=True),
        lax.all_gather(query_weight, ("sp", "fs"), axis=0, tiled=True),
        lax.all_gather(key_weight, ("sp", "fs"), axis=0, tiled=True),
        lax.all_gather(value_weight, ("sp", "fs"), axis=0, tiled=True),
    )
    projected = tuple(
        (jnp.dot(normed, fragment, preferred_element_type=jnp.float32) for fragment in fragments)
    )
    pool_in, queries, keys_flat, values_flat = [
        product.astype(jnp.bfloat16) for product in projected
    ]
    head_count = values_flat.shape[1] // (2 * HEAD_DIM)
    tp_index = lax.axis_index("tp")
    sp_index = lax.axis_index("sp")
    query_pos = sp_index * row_count + jnp.arange(row_count, dtype=jnp.int32)
    positions = query_pos.astype(jnp.float32)
    queries = rotate(queries.reshape(row_count, head_count, 2, HEAD_DIM), positions)
    keys_flat = rotate(keys_flat.reshape(row_count, head_count, 2, HEAD_DIM), positions).reshape(
        row_count, head_count * 2 * HEAD_DIM
    )
    lambdas = lax.dynamic_slice_in_dim(diff_lambda, tp_index * head_count, head_count, 0)

    def online_step(state, key_rows, value_rows, key_offset):
        largest, summed, accum = state
        width = key_rows.shape[0]
        shaped = key_rows.reshape(width, head_count, 2, HEAD_DIM)
        scores = jnp.einsum(
            "qhcd,khcd->chqk", queries, shaped, preferred_element_type=jnp.float32
        ) * HEAD_DIM ** (-0.5)
        key_pos = key_offset + jnp.arange(width, dtype=jnp.int32)
        scores = jnp.where(query_pos[:, None] >= key_pos[None, :], scores, -jnp.inf)
        newest = jnp.maximum(largest, jnp.max(scores, -1))
        anchor = jnp.where(jnp.isfinite(newest), newest, 0.0)
        rescale = jnp.exp(largest - anchor)
        expons = jnp.exp(scores - anchor[..., None])
        summed = summed * rescale + jnp.sum(expons, -1)
        value_shaped = value_rows.reshape(width, head_count, 2 * HEAD_DIM)
        added = jnp.einsum(
            "chqk,khe->chqe",
            expons.astype(jnp.bfloat16),
            value_shaped,
            preferred_element_type=jnp.float32,
        )
        accum = accum * rescale[..., None] + added
        return (newest, summed, accum)

    start_state = (
        jnp.full((2, head_count, row_count), -jnp.inf, jnp.float32),
        jnp.zeros((2, head_count, row_count), jnp.float32),
        jnp.zeros((2, head_count, row_count, 2 * HEAD_DIM), jnp.float32),
    )
    fragments = (
        lax.all_gather(keys_flat, "sp", axis=0, tiled=True),
        lax.all_gather(values_flat, "sp", axis=0, tiled=True),
    )
    span = math.gcd(fragments[0].shape[0], 1024)

    def inner_step(index, inner_state):
        key_rows = lax.dynamic_slice_in_dim(fragments[0], index * span, span, 0)
        value_rows = lax.dynamic_slice_in_dim(fragments[1], index * span, span, 0)
        return online_step(inner_state, key_rows, value_rows, index * span)

    final_state = lax.fori_loop(0, fragments[0].shape[0] // span, inner_step, start_state)
    summed_final = final_state[1]
    accum_final = final_state[2]
    heads_raw = (
        accum_final[0] / summed_final[0][..., None]
        - lambdas[:, None, None] * accum_final[1] / summed_final[1][..., None]
    )
    heads_raw = jnp.moveaxis(heads_raw, 0, 1)
    attn = (
        (
            heads_raw
            * lax.rsqrt(jnp.mean(heads_raw * heads_raw, -1, keepdims=True) + HEAD_EPS)
            * head_gain
            * HEAD_SCALE
        )
        .astype(jnp.bfloat16)
        .reshape(row_count, head_count * 2 * HEAD_DIM)
    )
    reach = 15
    rim_rows = from_behind(pool_in[row_count - reach :], "sp", 1)
    extended = jnp.concatenate([rim_rows, pool_in], 0).astype(jnp.float32)
    pair_sums = extended[1:] + extended[:-1]
    quad_sums = pair_sums[2:] + pair_sums[:-2]
    octet_sums = quad_sums[4:] + quad_sums[:-4]
    sixteen_sums = octet_sums[8:] + octet_sums[:-8]
    group_count = pool_in.shape[1] // GROUP_DIM
    stacked = jnp.stack(
        [
            pair_sums[14 : 14 + row_count],
            quad_sums[12 : 12 + row_count],
            octet_sums[8 : 8 + row_count],
            sixteen_sums,
        ],
        0,
    ).reshape(4, row_count, group_count, GROUP_DIM)
    levels = (tp_index * group_count + jnp.arange(group_count, dtype=jnp.int32)) % 4
    picked = jnp.sum(
        jnp.where(
            levels[None, None, :, None] == jnp.arange(4, dtype=jnp.int32)[:, None, None, None],
            stacked,
            0.0,
        ),
        0,
    )
    windows = 2 ** (1 + levels)
    counts = jnp.minimum(query_pos[:, None] + 1, windows[None, :]).astype(jnp.float32)
    window_mean = picked / counts[:, :, None]
    grouped = pool_in.reshape(row_count, group_count, GROUP_DIM).astype(jnp.float32)
    pool_mixed = (window_mean - grouped).astype(jnp.bfloat16)
    pooled = (
        (
            jnp.einsum("tgc,gce->tge", pool_mixed, pool_map, preferred_element_type=jnp.float32)
            * pool_scale.reshape(group_count, GROUP_DIM)
        )
        .astype(jnp.bfloat16)
        .reshape(row_count, group_count * GROUP_DIM)
    )
    branches = jnp.concatenate([pooled, attn], 1)
    partial_value = jnp.dot(
        branches,
        lax.all_gather(out_local, ("sp", "fs"), axis=1, tiled=True),
        preferred_element_type=jnp.float32,
    )
    layer_out = lax.psum_scatter(
        partial_value.astype(jnp.bfloat16), "tp", scatter_dimension=1, tiled=True
    )
    return layer_out[None]


VMEM = pl.BlockSpec(memory_space=pltpu.VMEM)
SMEM = pl.BlockSpec(memory_space=pltpu.SMEM)
HBM = pl.BlockSpec(memory_space=pltpu.HBM)
CHUNKS = 2
VMEM_LIMIT = 16 * 1024 * 1024
WHOLE_VMEM = 60 * 1024 * 1024


def call(kernel, outs, scratch, cost, specs, *args, limit=VMEM_LIMIT):
    flops, moved, exps = cost
    return pl.pallas_call(
        kernel,
        out_shape=[jax.ShapeDtypeStruct(shape, dtype) for shape, dtype in outs],
        in_specs=specs,
        out_specs=[VMEM] * len(outs),
        scratch_shapes=scratch,
        compiler_params=pltpu.CompilerParams(vmem_limit_bytes=limit),
        cost_estimate=pl.CostEstimate(flops=flops, bytes_accessed=moved, transcendentals=exps),
    )(*args)


def move(pairs_of, outs, count, *args, limit=VMEM_LIMIT):
    def kernel(*refs):
        sems = refs[-1]
        copies = [
            pltpu.make_async_copy(source, target, sems.at[i])
            for i, (source, target) in enumerate(pairs_of(refs[: len(args)], refs[len(args) : -1]))
        ]
        for copy in copies:
            copy.start()
        for copy in copies:
            copy.wait()

    moved = sum(2 * math.prod(shape) * 2 for shape, _ in outs)
    return call(
        kernel, outs, [pltpu.SemaphoreType.DMA((count,))], (0, moved, 0), [HBM] * len(args), *args,
        limit=limit,
    )


def place(pairs_of, outs, *args):
    def kernel(*refs):
        for source, target in pairs_of(refs[: len(args)], refs[len(args) :]):
            target[...] = source[...]

    moved = sum(2 * math.prod(shape) * 2 for shape, _ in outs)
    return call(kernel, outs, [], (0, moved, 0), [VMEM] * len(args), *args)


def tiles(start, size):
    return pl.ds(pl.multiple_of(start * size, size), size)


def project_kernel(slot, *refs):
    *xs, w_ref, turn_ref, out_ref = refs if slot == 0 else refs[:-1]
    rows = out_ref.shape[0]
    if slot:
        x_ref = refs[-1]
        tp = lax.axis_index("tp")
        size = xs[0].shape[0]
        each = len(xs) // 2
        for c in range(each):
            x_ref[tiles(tp * each + c, size)] = xs[c][...]
            x_ref[tiles((1 - tp) * each + c, size)] = xs[each + c][...]
    else:
        x_ref = xs[0]
    width = w_ref.shape[1] // 4
    table = turn_ref[tiles(lax.axis_index("sp") ^ slot, rows)]
    other = pltpu.roll(table, HEAD_DIM // 2, 1)
    front = lax.broadcasted_iota(jnp.int32, table.shape, 1) < HEAD_DIM // 2
    cosine, sine = jnp.where(front, table, other), jnp.where(front, -other, table)
    for part in range(4):
        product = jnp.dot(
            x_ref[...], w_ref[:, part * width : (part + 1) * width], preferred_element_type=jnp.float32
        ).astype(jnp.bfloat16)
        if part in (1, 2):
            raw = product.astype(jnp.float32)
            turned = [
                raw[:, m : m + HEAD_DIM] * cosine
                + pltpu.roll(raw[:, m : m + HEAD_DIM], HEAD_DIM // 2, 1) * sine
                for m in range(0, width, HEAD_DIM)
            ]
            product = jnp.concatenate(turned, 1).astype(jnp.bfloat16)
        out_ref[:, part * width : (part + 1) * width] = product


def mix_kernel(slot, total, part, parts, *refs):
    projs, (map_ref, scale_ref, gain_ref, lam_ref, w_ref, sent_ref, kept_ref, branch_ref) = (
        refs[:total],
        refs[total:],
    )
    rows = projs[0].shape[0]
    size = rows // parts
    first = part * size
    mine = slice(first, first + size)
    width = 2 * HEAD_DIM
    place = lax.axis_index("sp")
    group = lax.axis_index("tp") * total + place
    level = lax.rem(group, 4)
    block = place ^ slot
    scale = HEAD_DIM ** (-0.5)
    ahead = lax.broadcasted_iota(jnp.int32, (size, rows), 0) + first >= lax.broadcasted_iota(
        jnp.int32, (size, rows), 1
    )
    halves = []
    for m in range(2):
        begin = GROUP_DIM + m * HEAD_DIM
        query = projs[slot][mine, begin : begin + HEAD_DIM]
        scores, tops = [], []
        for j in range(total):
            score = lax.dot_general(
                query,
                projs[j][:, begin + width : begin + width + HEAD_DIM],
                (((1,), (1,)), ((), ())),
                preferred_element_type=jnp.float32,
            )
            if j == slot:
                score = jnp.where(ahead, score, -jnp.inf)
                tops.append(jnp.max(score, -1, keepdims=True))
            else:
                bias = jnp.where((place ^ j) < block, 0.0, -jnp.inf)
                tops.append(jnp.max(score, -1, keepdims=True) + bias)
            scores.append(score)
        largest = functools.reduce(jnp.maximum, tops)
        sums, summed = 0.0, 0.0
        for j in range(total):
            limit = largest
            if j != slot:
                limit = largest + jnp.where((place ^ j) < block, 0.0, jnp.inf)
            expons = jnp.exp((scores[j] - limit) * scale)
            sums = sums + jnp.sum(expons, -1, keepdims=True)
            summed = summed + jnp.dot(
                expons.astype(jnp.bfloat16),
                projs[j][:, GROUP_DIM + 2 * width :],
                preferred_element_type=jnp.float32,
            )
        halves.append(summed / sums)
    raw = halves[0] - lam_ref[group] * halves[1]
    attn = (
        raw
        * lax.rsqrt(jnp.mean(raw * raw, -1, keepdims=True) + HEAD_EPS)
        * gain_ref[...]
        * HEAD_SCALE
    ).astype(jnp.bfloat16)
    branch_ref[:, GROUP_DIM:] = attn

    reach = 16
    if first:
        rim = projs[slot][first - reach : first, :GROUP_DIM]
    else:
        rim = jnp.zeros((reach, GROUP_DIM), jnp.bfloat16)
        for j in range(total):
            rim = jnp.where((place ^ j) == block - 1, projs[j][rows - reach :, :GROUP_DIM], rim)
    flat = jnp.concatenate([rim, projs[slot][mine, :GROUP_DIM]], 0).astype(jnp.float32)
    sums = flat
    picked = jnp.zeros((size, GROUP_DIM), jnp.float32)
    for power in range(4):
        sums = sums + pltpu.roll(sums, 2**power, 0)
        picked = jnp.where(level == power, sums[reach:], picked)
    window = lax.shift_left(jnp.int32(2), level)
    own_pos = block * rows + first + lax.broadcasted_iota(jnp.int32, (size, GROUP_DIM), 0)
    counts = jnp.minimum(own_pos + 1, window).astype(jnp.float32)
    mixed = (picked / counts - flat[reach:]).astype(jnp.bfloat16)
    pooled = jnp.dot(mixed, map_ref[place], preferred_element_type=jnp.float32) * scale_ref[:, tiles(place, GROUP_DIM)]
    branch_ref[:, :GROUP_DIM] = pooled.astype(jnp.bfloat16)
    sent_ref[...] = jnp.dot(
        branch_ref[...], w_ref[1], preferred_element_type=jnp.float32
    ).astype(jnp.bfloat16)
    kept_ref[...] = jnp.dot(branch_ref[...], w_ref[0], preferred_element_type=jnp.float32)


def swap(value, axis, bits):
    return lax.ppermute(value, axis, [(i, i ^ bits) for i in range(lax.axis_size(axis))])


def after(value, *earlier):
    return lax.optimization_barrier((value, *earlier))[0]


def square(front, back):
    back_one, front_two = swap(back, "fs", 1), swap(front, "fs", 2)
    front_one, back_two = swap(front, "fs", 1), swap(back, "fs", 2)
    front_three = swap(front_two, "fs", 1)
    back_three = swap(back_one, "fs", 2)
    return [(front, back), (front_one, back_one), (front_two, back_two), (front_three, back_three)]


def spread(
    tokens,
    norm_gain,
    pool_input,
    query_weight,
    key_weight,
    value_weight,
    pool_map,
    pool_scale,
    head_gain,
    diff_lambda,
    out_pool,
    out_heads,
):
    low, wide = jnp.bfloat16, jnp.float32
    n_sp, n_fs, n_tp = (lax.axis_size(axis) for axis in ("sp", "fs", "tp"))
    tp = lax.axis_index("tp")
    rows, depth = tokens.shape[1:]
    shard = depth // (n_sp * n_fs)
    channels = GROUP_DIM + 2 * HEAD_DIM
    width = GROUP_DIM + 3 * 2 * HEAD_DIM
    part = width // 4

    def columns(sources, targets):
        sp = lax.axis_index("sp")
        return [
            (source.at[:, tiles(sp ^ j, part)], targets[j].at[:, i * part : (i + 1) * part])
            for j in (*range(n_sp - 1, 0, -1), 0)
            for i, source in enumerate(sources)
        ]

    pieces = move(
        columns, [((shard, width), low)] * n_sp, 4 * n_sp,
        pool_input, query_weight, key_weight, value_weight, limit=WHOLE_VMEM,
    )
    near = [pieces[0]] + [swap(pieces[0], "fs", i) for i in range(1, n_fs)]
    far = [swap(pieces[j], "sp", j) for j in range(1, n_sp)]
    half_shard = shard // 2

    def bundle(sources, targets):
        return [
            (source.at[tiles(side, half_shard)], targets[side].at[tiles(i, half_shard)])
            for side in range(2)
            for i, source in enumerate(sources)
        ]

    bundled = place(bundle, [(((n_sp - 1) * half_shard, width), low)] * 2, *far)
    distant = [part for pair in square(*bundled) for part in pair]

    def assemble(sources, targets):
        sp, fs = lax.axis_index("sp"), lax.axis_index("fs")
        pairs = []
        for i in range(n_fs):
            pairs.append((sources[i], targets[0].at[tiles(sp * n_fs + (fs ^ i), shard)]))
            for j in range(1, n_sp):
                place = (sp ^ j) * n_fs + (fs ^ i)
                for side in range(2):
                    source = sources[n_fs + 2 * i + side].at[tiles(j - 1, half_shard)]
                    pairs.append((source, targets[0].at[tiles(2 * place + side, half_shard)]))
        return pairs

    (weight,) = place(assemble, [((depth, width), low)], *near, *distant)

    size = channels // 2

    def rows_of(steps):
        def pairs(sources, targets):
            sp = lax.axis_index("sp")
            return [
                (source.at[tiles(sp ^ j, size)], target.at[tiles(i, size)])
                for j, target in zip(steps, targets, strict=True)
                for i, source in enumerate(sources)
            ]

        return move(
            pairs, [((channels, shard), low)] * len(steps), 2 * len(steps),
            out_pool, out_heads, limit=WHOLE_VMEM,
        )

    pieces_out = rows_of((3, 2)) + rows_of((1, 0))
    pieces_out = pieces_out[::-1]
    far_out = [pieces_out[0]] + [swap(pieces_out[j], "sp", j) for j in range(1, n_sp)]

    def bundle_out(sources, targets):
        return [
            (source.at[tiles(side, size)], targets[side].at[tiles(j, size)])
            for side in range(2)
            for j, source in enumerate(sources)
        ]

    bundled_out = place(bundle_out, [((n_sp * size, shard), low)] * 2, *far_out)

    def assemble_out(sources, targets):
        sp, fs, tp = (lax.axis_index(axis) for axis in ("sp", "fs", "tp"))
        per = n_sp // n_tp
        pairs = []
        for i in range(n_fs):
            for j in range(n_sp):
                other = sp ^ j
                here = tiles(lax.rem(other, per) * n_fs + (fs ^ i), shard)
                target = targets[0].at[lax.div(other, per) ^ tp]
                for side in range(2):
                    source = sources[2 * i + side].at[tiles(j, size)]
                    pairs.append((source, target.at[tiles(side, size), here]))
        return pairs

    (out_weight,) = place(
        assemble_out, [((n_tp, channels, depth // n_tp), low)],
        *[part for pair in square(*bundled_out) for part in pair],
    )

    floated = tokens[0].astype(wide)
    own = (
        floated * lax.rsqrt(jnp.mean(floated * floated, -1, keepdims=True) + NORM_EPS) * norm_gain
    ).astype(low)
    half = rows // n_tp
    size_of = half // CHUNKS
    mine = [
        lax.dynamic_slice_in_dim(own, tp * half + c * size_of, size_of, 0) for c in range(CHUNKS)
    ]
    whole = lax.dynamic_slice_in_dim(own, tp * half, half, 0)
    slots = {1: [swap(whole, "sp", 1)]}
    slots[2] = [swap(piece, "sp", 2) for piece in mine]
    slots[3] = [swap(piece, "sp", 1) for piece in slots[2]]

    half_dim = HEAD_DIM // 2
    freqs = 1.0 / THETA ** (np.arange(half_dim, dtype=np.float32) * 2.0 / HEAD_DIM)
    angles = np.arange(rows * n_sp, dtype=np.float64)[:, None] * freqs[None, :]
    table = jnp.asarray(np.concatenate([np.cos(angles), np.sin(angles)], 1).astype(np.float32))

    def project(j):
        xs = [own]
        if j:
            xs = slots[j] + [swap(piece, "tp", 1) for piece in slots[j]]
        scratch = [pltpu.VMEM((rows, depth), low)] if j else []
        return call(
            functools.partial(project_kernel, j), [((rows, width), low)], scratch,
            (2 * rows * depth * width, 2 * depth * width, 0), [VMEM] * (len(xs) + 2),
            *xs, weight, table,
        )[0]

    projs = [project(j) for j in range(n_sp)]
    gain = head_gain[None]

    def mixed(slot, gain, part=0, parts=1):
        size = rows // parts
        sent, kept = call(
            functools.partial(mix_kernel, slot, n_sp, part, parts),
            [((size, depth // n_tp), low), ((size, depth // n_tp), wide)],
            [pltpu.VMEM((size, channels), low)],
            (8 * size * rows * n_sp * HEAD_DIM + 2 * size * channels * depth, 8 * rows * width + 2 * depth * channels,
             2 * size * rows * n_sp),
            [VMEM] * (n_sp + 3) + [SMEM, VMEM],
            *projs, pool_map, pool_scale[None], gain, diff_lambda, out_weight,
        )
        return kept, swap(sent, "tp", 1)

    def total(parts, c=None, *more):
        if c is not None:
            parts = [part[c * half : (c + 1) * half] for part in parts]
        return sum(part.astype(wide) for part in (*parts, *more))

    early = mixed(3, gain, 0, 2)
    late = mixed(3, after(gain, early[0]), 1, 2)
    sum_three = total(early).astype(low)
    from_three = [swap(sum_three, "sp", 1)]
    gain = after(gain, late[0], sum_three)
    two = mixed(2, gain)
    from_three.append(swap(after(total(late).astype(low), two[0]), "sp", 1))
    one = mixed(1, gain)
    sum_two = [total(two, 0, from_three[0]).astype(low)]
    sum_two.append(total(two, 1, after(from_three[1], sum_two[0])).astype(low))
    from_two = [swap(sum_two[c], "sp", 2) for c in range(2)]
    zero = mixed(0, gain)
    from_one = swap(total(one).astype(low), "sp", 1)
    result = [total((*zero, from_one), c, from_two[c]).astype(low) for c in range(2)]
    return jnp.concatenate(result, 0)[None]


def solution(mesh):
    placed = (
        P("fs", "sp", None),
        P(),
        P(("sp", "fs"), "tp"),
        P(("sp", "fs"), "tp"),
        P(("sp", "fs"), "tp"),
        P(("sp", "fs"), "tp"),
        P("tp", None, None),
        P("tp"),
        P(),
        P(),
        P("tp", ("sp", "fs")),
        P("tp", ("sp", "fs")),
    )

    def body(*args):
        n_sp, n_fs, n_tp = (mesh.shape[axis] for axis in ("sp", "fs", "tp"))
        groups, heads = args[6].shape[0], args[5].shape[1] // (2 * HEAD_DIM)
        pairs = groups == heads == n_sp == n_fs == 4 and n_tp == 2
        return (spread if pairs else local)(*args)

    return jax.shard_map(
        body, mesh=mesh, in_specs=placed, out_specs=P("fs", "sp", "tp"), check_vma=False
    )
```
